256 devices in a mesh: fs: 64 (over z, x, core), tp: 4 (over y).
Axes of the slice: x: 4, y: 4, z: 8, core: 2. Of those that a mesh axis runs over, the one named last changes fastest.
Arguments:
- tokens: bfloat16 [768, 4, 2048], P(None, 'tp'), may hold values from -6 to 6
- norm_gain: float32 [2048], P('fs'), may hold values from 0.1 to 1.9
- gate_weight: float32 [8, 2048, 4096], P(None, 'fs', 'tp'), may hold values from -0.125 to 0.125
- up_weight: float32 [8, 2048, 4096], P(None, 'fs', 'tp'), may hold values from -0.125 to 0.125
- down_weight: float32 [8, 2048, 4096], P(None, 'fs', 'tp'), may hold values from -0.09375 to 0.09375
- expert_ids: int32 [768, 4, 2], P(None, 'tp'), may hold values from 0 to 7, all different within a row
- expert_mix: float32 [768, 4, 2], P(None, 'tp'), may hold values from 0.2 to 1
Outputs:
- gate_serve: bfloat16 [8, 2048, 4096], P(None, None, 'fs')
- up_serve: bfloat16 [8, 2048, 4096], P(None, None, 'fs')
- down_serve: bfloat16 [8, 2048, 4096], P(None, None, 'fs')
- mixed: bfloat16 [768, 4, 2048], P('fs', 'tp')
The draws below stay inside these ranges and needn't reach their ends.
Inputs may be any that keep to these rules, and one draw needn't show every extreme that they name: `expert_ids`: each token names two different experts.
All inputs are finite; a program needn't handle non-finite values.
Results may differ from the reference program's by a relative error of at most 0.0082.
Values may be sent and summed in bfloat16 or wider, within the bound.
A program may use at most 64 MiB of HBM per device.

```python
import jax
import jax.numpy as jnp
from jax import lax

D = 2048
FF = 4096
EXPERTS = 8
ROWS = 768
N_TP = 4


def shard_levels(rng, shape, pieces, smallest, top_value):
    gain, own = 1.0, jax.random.fold_in(rng, 6)
    for axis_at, parts in pieces:
        heights = jnp.exp(jax.random.uniform(jax.random.fold_in(own, axis_at), (parts,), jnp.float32, smallest / len(pieces), top_value / len(pieces)))
        gain = gain * jnp.repeat(heights, shape[axis_at] // parts).reshape([-1 if axis == axis_at else 1 for axis in range(len(shape))])
    return gain


def picks_of(key, rows, count, top, lift):
    order = jax.random.permutation(jax.random.fold_in(key, 1), count)
    pull = order
    for power in range(3):
        pull = pull * pull // count
    pull = pull * lift // count
    tickets = jax.random.randint(jax.random.fold_in(key, 2), (rows, count), 0, 4096) + pull
    fixed_rows = jax.random.permutation(jax.random.fold_in(key, 3), rows)[jnp.arange(count) % rows]
    tickets = jnp.where(jnp.arange(rows)[:, None] == fixed_rows[None, :], 1 << 14, tickets)
    priority = tickets * count + jnp.arange(count)
    return lax.top_k(priority.astype(jnp.int32), top)[1].astype(jnp.int32)


def normal_values(rng, dims, deviation, reach, pieces=(), held_as=jnp.bfloat16):
    entries = jax.random.normal(rng, dims, jnp.float32) * deviation
    if len(pieces) > 0:
        entries = shard_levels(rng, dims, pieces, -0.22, 0.18) * entries
    return jnp.clip(entries, min=-reach, max=reach).astype(held_as)


def setup_inputs(seed: int = 0) -> dict:
    key_of = jax.random.split(jax.random.key(seed), 8)
    tokens = normal_values(key_of[0], (ROWS, N_TP, D), 1.0, 6.0, ((1, 4),))
    norm_gain = jnp.clip(1.0 + 0.18 * jax.random.normal(key_of[1], (D,), jnp.float32), 0.1, 1.9)
    gate_weight = normal_values(key_of[2], (EXPERTS, D, FF), D ** -0.5, 0.125, ((1, 64), (2, 4)), jnp.float32)
    up_weight = normal_values(key_of[3], (EXPERTS, D, FF), D ** -0.5, 0.125, ((1, 64), (2, 4)), jnp.float32)
    down_weight = normal_values(key_of[4], (EXPERTS, D, FF), FF ** -0.5, 0.09375, ((1, 64), (2, 4)), jnp.float32)
    expert_ids = picks_of(key_of[5], ROWS * N_TP, EXPERTS, 2, 0).reshape((ROWS, N_TP, 2))
    expert_mix = jnp.clip(0.2 + 0.8 * jax.random.uniform(key_of[6], (ROWS, N_TP, 2), jnp.float32) ** shard_levels(key_of[6], (ROWS, N_TP, 2), ((1, 4),), -0.2, 0.2), 0.2, 1.0)
    return dict(tokens=tokens, norm_gain=norm_gain, gate_weight=gate_weight, up_weight=up_weight, down_weight=down_weight, expert_ids=expert_ids, expert_mix=expert_mix)


norm_eps = 1e-05

def reference(tokens, norm_gain, gate_weight, up_weight, down_weight, expert_ids, expert_mix):
    gate_serve = (gate_weight * norm_gain[None, :, None]).astype(jnp.bfloat16)
    up_serve = (up_weight * norm_gain[None, :, None]).astype(jnp.bfloat16)
    down_serve = down_weight.astype(jnp.bfloat16)
    token_rows = tokens.reshape(-1, D).astype(jnp.float32)
    row_mean = lax.optimization_barrier(jnp.mean(token_rows, axis=1, keepdims=True))
    centered = token_rows - row_mean
    variance = lax.optimization_barrier(jnp.mean(centered * centered, axis=1, keepdims=True))
    normed = (centered * lax.rsqrt(variance + norm_eps)).astype(jnp.bfloat16)
    route_ids = expert_ids.reshape(-1, 2)
    route_mix = expert_mix.reshape(-1, 2)
    expert_iota = jnp.arange(EXPERTS, dtype=jnp.int32)
    expert_gates = lax.optimization_barrier(jnp.sum((route_ids[:, :, None] == expert_iota[None, None, :]).astype(jnp.float32) * route_mix[:, :, None], axis=1))

    def add_expert(running, weights_now):
        gate_mat, up_mat, down_mat, gate_col = weights_now
        gate_act = jnp.dot(normed, gate_mat, preferred_element_type=jnp.float32)
        up_act = jnp.dot(normed, up_mat, preferred_element_type=jnp.float32)
        hidden = (jax.nn.silu(gate_act) * up_act * gate_col[:, None]).astype(jnp.bfloat16)
        product = lax.dot_general(hidden, down_mat, (((1,), (1,)), ((), ())), preferred_element_type=jnp.float32)
        return (running + product, None)
    start_sum = jnp.zeros((token_rows.shape[0], D), jnp.float32)
    summed, _ = lax.scan(add_expert, start_sum, (gate_serve, up_serve, down_serve, expert_gates.T))
    mixed = summed.astype(jnp.bfloat16).reshape(ROWS, N_TP, D)
    return (gate_serve, up_serve, down_serve, mixed)
```

```python
import jax
import jax.numpy as jnp
from jax import lax
from jax.experimental import pallas as pl
from jax.experimental.pallas import tpu as pltpu
from jax.sharding import Mesh
from jax.sharding import PartitionSpec as P

FS = ("fs_0", "fs_1", "fs_2")
NZ, NX, NC, NY = 8, 4, 2, 4
norm_eps = 1e-05
BF, F32 = jnp.bfloat16, jnp.float32
MESH = pl.DeviceIdType.MESH

CHUNKS = ((0, 0), (1, 0), (0, 1), (1, 1), (2, 0), (2, 1))
NQ = len(CHUNKS)


def send(src, dst, send_sem, recv_sem, to):
    pltpu.make_async_remote_copy(
        src_ref=src, dst_ref=dst, send_sem=send_sem, recv_sem=recv_sem, device_id=to, device_id_type=MESH
    ).start()


def wait_bytes(ref, sem):
    pltpu.make_async_copy(ref, ref, sem).wait()


def greet(z, x, c, y, along_y):
    barrier = pltpu.get_barrier_semaphore()
    count = 0
    me = 2 * x + c
    for off in range(1, NX * NC):
        j = lax.rem(me + off, NX * NC)
        pl.semaphore_signal(
            barrier, inc=1, device_id={"fs_1": j // 2, "fs_2": lax.rem(j, 2)}, device_id_type=MESH
        )
        count += 1
    for off in range(1, NZ):
        pl.semaphore_signal(barrier, inc=1, device_id={"fs_0": lax.rem(z + off, NZ)}, device_id_type=MESH)
        count += 1
    if along_y:
        for off in (1, NY - 1):
            pl.semaphore_signal(barrier, inc=1, device_id={"tp": lax.rem(y + off, NY)}, device_id_type=MESH)
            count += 1
    pl.semaphore_wait(barrier, count)


def weights_kernel(
    gate, up, down, gain, og, ou, od,
    xs, xr, ts, az, fw, w,
    x_send, x_recv, a_send, a_recv, f_send, f_recv, z_send, z_recv, c_send, c_recv, g_send, g_recv, o_sem,
):
    z, x, c, y = (lax.axis_index(a) for a in ("fs_0", "fs_1", "fs_2", "tp"))
    me = 2 * x + c
    ahead, behind, across = (lax.rem(y + o, NY) for o in (1, 3, 2))
    mats, outs = (gate, up, down), (og, ou, od)
    column = pl.multiple_of(256 * z, 256)
    greet(z, x, c, y, True)

    def pack(q):
        m, el = CHUNKS[q]
        low = lax.broadcasted_iota(jnp.int32, (32, 128), 1) < 64

        def one(i, carry):
            ep, xp = i // NX, lax.rem(i, NX)
            left = pl.multiple_of(128 * xp, 128)
            a = mats[m][2 * ep + el, :, pl.ds(left, 128)]
            b = mats[m][2 * ep + el, :, pl.ds(pl.multiple_of(512 + left, 128), 128)]
            if m < 2:
                a, b = a * gain[...], b * gain[...]
            xs[q, 2 * xp, ep] = jnp.where(low, a, pltpu.roll(b, 64, 1)).astype(BF)
            xs[q, 2 * xp + 1, ep] = jnp.where(low, pltpu.roll(a, 64, 1), b).astype(BF)
            return carry

        lax.fori_loop(0, 4 * NX, one, 0)
        for off in range(1, NX * NC):
            j = lax.rem(me + off, NX * NC)
            send(
                xs.at[q, j], xr.at[q, me], x_send.at[q], x_recv.at[q],
                {"fs_1": j // 2, "fs_2": lax.rem(j, 2)},
            )
        xr[q, me] = xs[q, me]

    def turn(q):
        wait_bytes(xr.at[q, 0:7], x_recv.at[q])

        def one(ep, carry):
            for h in range(2):
                rows = jnp.concatenate([xr[q, 4 * h + k, ep] for k in range(4)], axis=0)
                ts[q, ep, :, 128 * h : 128 * (h + 1)] = rows.T
            return carry

        lax.fori_loop(0, 4, one, 0)
        send(ts.at[q, across, 0:64], fw.at[q, 0], a_send.at[q], f_recv.at[q, 0], {"tp": ahead})
        send(ts.at[q, across, 64:128], fw.at[q, 1], a_send.at[q], f_recv.at[q, 1], {"tp": behind})
        send(ts.at[q, ahead], az.at[q, y], a_send.at[q], a_recv.at[q], {"tp": ahead})
        send(ts.at[q, behind], az.at[q, y], a_send.at[q], a_recv.at[q], {"tp": behind})
        az[q, y] = ts[q, y]

    def relay(q):
        wait_bytes(fw.at[q, 0], f_recv.at[q, 0])
        send(fw.at[q, 0], az.at[q, behind, 0:64], f_send.at[q], a_recv.at[q], {"tp": ahead})
        wait_bytes(fw.at[q, 1], f_recv.at[q, 1])
        send(fw.at[q, 1], az.at[q, ahead, 64:128], f_send.at[q], a_recv.at[q], {"tp": behind})

    def along_z(q):
        wait_bytes(az.at[q, 0:3], a_recv.at[q])
        for off in (4, 3, 5, 2, 6, 1, 7):
            zp = lax.rem(z + off, NZ)
            rows = pl.multiple_of(64 * lax.rem(zp, 2), 64)
            send(
                az.at[q, zp // 2, pl.ds(rows, 64), :], w.at[q, y, :, pl.ds(column, 256)],
                z_send.at[q], z_recv.at[q], {"fs_0": zp},
            )
        rows = pl.multiple_of(64 * lax.rem(z, 2), 64)
        w[q, y, :, pl.ds(column, 256)] = az[q, z // 2, pl.ds(rows, 64), :]

    def spread(q):
        wait_bytes(w.at[q, 0, :, 0:1792], z_recv.at[q])
        send(w.at[q, y], w.at[q, y], c_send.at[q], c_recv.at[q, 0], {"tp": ahead})
        send(w.at[q, y], w.at[q, y], c_send.at[q], c_recv.at[q, 1], {"tp": behind})

    def spread_on(q):
        wait_bytes(w.at[q, behind], c_recv.at[q, 0])
        send(w.at[q, behind, 0:32], w.at[q, behind, 0:32], g_send.at[q], g_recv.at[q], {"tp": ahead})
        wait_bytes(w.at[q, ahead], c_recv.at[q, 1])
        send(w.at[q, ahead, 32:64], w.at[q, ahead, 32:64], g_send.at[q], g_recv.at[q], {"tp": behind})

    def put_out(q):
        m, el = CHUNKS[q]
        wait_bytes(w.at[q, across], g_recv.at[q])
        for ep in range(4):
            pltpu.make_async_copy(w.at[q, ep], outs[m].at[2 * ep + el], o_sem.at[q]).start()

    stages = (pack, turn, relay, along_z, spread, spread_on, put_out)
    for q in range(NQ):
        pack(q)
    order = []
    for q in range(NQ):
        order += [(2.8 * q + 5, 1, q), (2.8 * q + 9, 2, q), (2.8 * q + 12, 3, q), (max(5.6 * q + 20, 8.5 * q + 18), 4, q)]
        order += [(11.2 * q + 32, 5, q), (11.2 * q + 40, 6, q)]
    for _, s, q in sorted(order):
        stages[s](q)
    for q in range(NQ):
        wait_bytes(xr.at[q, 0:7], x_send.at[q])
        wait_bytes(az.at[q, 0:3], a_send.at[q])
        wait_bytes(az.at[q, 0], f_send.at[q])
        wait_bytes(w.at[q, 0, :, 0:1792], z_send.at[q])
        wait_bytes(w.at[q, 0:2], c_send.at[q])
        wait_bytes(w.at[q, 0], g_send.at[q])
        wait_bytes(w.at[q], o_sem.at[q])


def move_weights(gate, up, down, gain):
    out = jax.ShapeDtypeStruct((8, 64, 2048), BF)
    vmem = pl.BlockSpec(memory_space=pltpu.VMEM)
    hbm = pl.BlockSpec(memory_space=pl.ANY)
    dma = pltpu.SemaphoreType.DMA
    return pl.pallas_call(
        weights_kernel,
        out_shape=(out, out, out),
        in_specs=[vmem] * 4,
        out_specs=(hbm, hbm, hbm),
        scratch_shapes=[
            pltpu.VMEM((NQ, 8, 4, 32, 128), BF),
            pltpu.VMEM((NQ, 8, 4, 32, 128), BF),
            pltpu.VMEM((NQ, 4, 128, 256), BF),
            pltpu.VMEM((NQ, 4, 128, 256), BF),
            pltpu.VMEM((NQ, 2, 64, 256), BF),
            pltpu.VMEM((NQ, 4, 64, 2048), BF),
            dma((NQ,)), dma((NQ,)),
            dma((NQ,)), dma((NQ,)),
            dma((NQ,)), dma((NQ, 2)),
            dma((NQ,)), dma((NQ,)),
            dma((NQ,)), dma((NQ, 2)),
            dma((NQ,)), dma((NQ,)),
            dma((NQ,)),
        ],
        compiler_params=pltpu.CompilerParams(
            collective_id=0, has_side_effects=True, vmem_limit_bytes=40 * 1024 * 1024
        ),
        name="move_weights",
    )(gate, up, down, gain)


BLOCK = 96
OFFSETS = (4, 3, 5, 2, 6, 1, 7, 0)


def sum_kernel(
    p, out, r1, s1, r2, s2, r3, s4, r4,
    send1, recv1, send2, recv2, send3, recv3, send4, recv4,
):
    z, x, c, y = (lax.axis_index(a) for a in ("fs_0", "fs_1", "fs_2", "tp"))
    mine, theirs = pl.multiple_of(1024 * c, 1024), pl.multiple_of(1024 * (1 - c), 1024)
    greet(z, x, c, y, False)

    def rows_of(k):
        zp = lax.rem(z + OFFSETS[k], NZ)
        return zp, pl.ds(pl.multiple_of(BLOCK * zp, BLOCK), BLOCK)

    def between_cores(k):
        _, rows = rows_of(k)
        send(p.at[rows, pl.ds(theirs, 1024)], r1.at[k], send1.at[k], recv1.at[k], {"fs_2": 1 - c})

    def along_x(k):
        _, rows = rows_of(k)
        wait_bytes(r1.at[k], recv1.at[k])
        total = p[rows, pl.ds(mine, 1024)].astype(F32) + r1[k].astype(F32)
        total = total.astype(BF)
        for xp in range(NX):
            s1[k, xp] = total[:, 256 * xp : 256 * (xp + 1)]
        for off in (2, 1, 3):
            xp = lax.rem(x + off, NX)
            send(s1.at[k, xp], r2.at[k, x], send2.at[k], recv2.at[k], {"fs_1": xp})
        r2[k, x] = s1[k, x]

    def along_z(k):
        zp, _ = rows_of(k)
        wait_bytes(r2.at[k, 0:3], recv2.at[k])
        total = (r2[k, 0].astype(F32) + r2[k, 1].astype(F32)) + (r2[k, 2].astype(F32) + r2[k, 3].astype(F32))
        if OFFSETS[k] == 0:
            r3[z] = total.astype(BF)
        else:
            s2[k] = total.astype(BF)
            send(s2.at[k], r3.at[z], send3.at[k], recv3, {"fs_0": zp})

    for k in range(NZ):
        between_cores(k)
    for k in range(NZ + 1):
        if k < NZ:
            along_x(k)
        if k > 0:
            along_z(k - 1)
    wait_bytes(r3.at[0:7], recv3)
    total = r3[0].astype(F32)
    for i in range(1, NZ):
        total = total + r3[i].astype(F32)
    row = lax.broadcasted_iota(jnp.int32, (128, BLOCK), 0)
    col = lax.broadcasted_iota(jnp.int32, (128, BLOCK), 1)
    within = lax.rem(row, 16)
    pick = ((col == (row // 16) * 12 + within) & (within < 12)).astype(BF)
    s4[...] = jnp.dot(pick, total.astype(BF), preferred_element_type=F32).astype(BF)
    me = 2 * x + c
    column = pl.multiple_of(256 * (4 * c + x), 256)
    for off in range(1, NX * NC):
        j = lax.rem(me + off, NX * NC)
        send(
            s4.at[pl.ds(pl.multiple_of(16 * j, 16), 16), :], r4.at[:, pl.ds(column, 256)],
            send4, recv4, {"fs_1": j // 2, "fs_2": lax.rem(j, 2)},
        )
    r4[:, pl.ds(column, 256)] = s4[pl.ds(pl.multiple_of(16 * me, 16), 16), :]
    wait_bytes(r4.at[:, 0:1792], recv4)
    out[...] = r4[0:12, :]
    for k in range(NZ):
        wait_bytes(r1.at[k], send1.at[k])
        wait_bytes(r2.at[k, 0:3], send2.at[k])
        if OFFSETS[k] != 0:
            wait_bytes(s2.at[k], send3.at[k])
    wait_bytes(r4.at[:, 0:1792], send4)


def sum_partials(p):
    vmem = pl.BlockSpec(memory_space=pltpu.VMEM)
    dma = pltpu.SemaphoreType.DMA
    return pl.pallas_call(
        sum_kernel,
        out_shape=jax.ShapeDtypeStruct((12, 2048), BF),
        in_specs=[vmem],
        out_specs=vmem,
        scratch_shapes=[
            pltpu.VMEM((NZ, BLOCK, 1024), BF),
            pltpu.VMEM((NZ, NX, BLOCK, 256), BF),
            pltpu.VMEM((NZ, NX, BLOCK, 256), BF),
            pltpu.VMEM((NZ, BLOCK, 256), BF),
            pltpu.VMEM((NZ, BLOCK, 256), BF),
            pltpu.VMEM((128, 256), BF),
            pltpu.VMEM((16, 2048), BF),
            dma((NZ,)), dma((NZ,)),
            dma((NZ,)), dma((NZ,)),
            dma((NZ,)), dma,
            dma, dma,
        ],
        compiler_params=pltpu.CompilerParams(
            collective_id=1, has_side_effects=True, vmem_limit_bytes=40 * 1024 * 1024
        ),
        name="sum_partials",
    )(p)


def local(tokens, norm_gain, gate_weight, up_weight, down_weight, expert_ids, expert_mix):
    gain = jnp.broadcast_to(norm_gain[:, None], (32, 128))
    gate_t, up_t, down_t = move_weights(gate_weight, up_weight, down_weight, gain)
    width = tokens.shape[2]
    token_rows = tokens.reshape(-1, width).astype(F32)
    row_mean = jnp.mean(token_rows, axis=1, keepdims=True)
    centered = token_rows - row_mean
    variance = jnp.mean(centered * centered, axis=1, keepdims=True)
    normed = (centered * lax.rsqrt(variance + norm_eps)).astype(BF)
    route_ids = expert_ids.reshape(-1, 2)
    route_mix = expert_mix.reshape(-1, 2)
    expert_iota = jnp.arange(8, dtype=jnp.int32)
    expert_gates = jnp.sum(
        (route_ids[:, :, None] == expert_iota[None, None, :]).astype(F32) * route_mix[:, :, None], axis=1
    )
    flat = (512, width)
    contract = (((1,), (1,)), ((), ()))
    gate_act = lax.dot_general(normed, gate_t.reshape(flat), contract, preferred_element_type=F32)
    up_act = lax.dot_general(normed, up_t.reshape(flat), contract, preferred_element_type=F32)
    hidden = (jax.nn.silu(gate_act) * up_act * jnp.repeat(expert_gates, 64, axis=1)).astype(BF)
    partial = jnp.dot(hidden, down_t.reshape(flat), preferred_element_type=F32).astype(BF)
    mixed = sum_partials(partial).reshape(-1, 1, width)
    turned = tuple(jnp.swapaxes(t, 1, 2) for t in (gate_t, up_t, down_t))
    return turned + (mixed,)


def solution(mesh):
    finer = Mesh(mesh.devices.reshape(NZ, NX, NC, NY), ("fs_0", "fs_1", "fs_2", "tp"))
    placed = (
        P(None, "tp", None),
        P(FS),
        P(None, FS, "tp"),
        P(None, FS, "tp"),
        P(None, FS, "tp"),
        P(None, "tp", None),
        P(None, "tp", None),
    )
    return jax.shard_map(
        local,
        mesh=finer,
        in_specs=placed,
        out_specs=(P(None, None, FS), P(None, None, FS), P(None, None, FS), P(FS, "tp", None)),
        check_vma=False,
    )
```

```python
import jax
import jax.numpy as jnp
from jax import lax
from jax.experimental import pallas as pl
from jax.experimental.pallas import tpu as pltpu
from jax.sharding import Mesh
from jax.sharding import PartitionSpec as P

FS = ("fs_0", "fs_1", "fs_2")
NZ, NX, NC, NY = 8, 4, 2, 4
norm_eps = 1e-05
BF, F32 = jnp.bfloat16, jnp.float32
MESH = pl.DeviceIdType.MESH

CHUNKS = ((0, 0), (1, 0), (0, 1), (1, 1), (2, 0), (2, 1))
NQ = len(CHUNKS)
ROWS, WIDTH, TILE = 768, 2048, 256
BLOCK = ROWS // NZ
PIECES = 4
PIECE = WIDTH // PIECES
PASSES = 2
LANES = WIDTH // PASSES
BY_CORE = LANES // NC
BY_X = BY_CORE // NX
PAIRS = (2, 1, 3, 0)
NP = len(PAIRS)
ORDER = (
    "A0 A1 R0 A2", "R1 A3 X0 R2", "A4 X1 R3 A5", "X2 Z0 R4 X3",
    "Z1 R5 X4 X5", "Z2 N0 S0", "N1 N2 N3 N4", "Z3 N5 N6 N7", "N8 Z4 S1 F0",
    "N9 N10 N11 Z5", "S2 F1 P0", "S3 F2 P1", "H0,0 H0,1 H0,2",
    "T0 T1 F3 P2", "U0 U1 T2 T3", "P3 H1,0 H1,1 H1,2", "V0 V1 B0,0 B0,1",
    "U2 C0,0 B0,2 C0,1", "B0,3 C0,2 C0,3 U3", "D0,0 D0,1 V2 V3",
    "B1,0 E0,0 B1,1 D0,2", "E0,1 B1,2 C1,0 D0,3", "B1,3 C1,1 E0,2 C1,2",
    "C1,3 E0,3 D1,0 D1,1", "G0 E1,0 D1,2 E1,1", "D1,3 E1,2 E1,3 G1",
)


def send(src, dst, send_sem, recv_sem, to):
    pltpu.make_async_remote_copy(
        src_ref=src, dst_ref=dst, send_sem=send_sem, recv_sem=recv_sem, device_id=to, device_id_type=MESH
    ).start()


def wait_bytes(ref, sem):
    pltpu.make_async_copy(ref, ref, sem).wait()


def kernel(
    tokens, ids, mix, gain, gate, up, down,
    og, ou, od, out,
    mat, tok, xs, ar, fw, xr, ts, w, xn, gates, h,
    pb, own, r1, s1, t2, u2, r2, s2, r3, s4, r4,
    in_sem, a_send, a_recv, f_send, f_recv, x_send, x_recv, z_send, z_recv,
    c_send, c_recv, g_send, g_recv, o_sem,
    send1, recv1, send2, recv2, sendt, recvt, send3, recv3, send4, recv4,
):
    z, x, c, y = (lax.axis_index(a) for a in ("fs_0", "fs_1", "fs_2", "tp"))
    me = 2 * x + c
    ahead, behind, across = (lax.rem(y + o, NY) for o in (1, 3, 2))
    right, left, opposite = (lax.rem(x + o, NX) for o in (1, 3, 2))
    column = pl.multiple_of(256 * z, 256)

    reads = [pltpu.make_async_copy(r, mat.at[m], in_sem.at[m]) for m, r in enumerate((gate, up, down))]
    reads.append(pltpu.make_async_copy(tokens, tok, in_sem.at[3]))
    for r in reads:
        r.start()

    barrier = pltpu.get_barrier_semaphore()
    peers = []
    for off in range(1, NX * NC):
        j = lax.rem(me + off, NX * NC)
        peers.append({"fs_1": j // 2, "fs_2": lax.rem(j, 2)})
    for off in range(1, NZ):
        peers.append({"fs_0": lax.rem(z + off, NZ)})
    peers += [{"tp": ahead}, {"tp": behind}]
    for to in peers:
        pl.semaphore_signal(barrier, inc=1, device_id=to, device_id_type=MESH)

    def pack(q):
        m, el = CHUNKS[q]
        low = lax.broadcasted_iota(jnp.int32, (32, 128), 1) < 64
        eye = lax.broadcasted_iota(jnp.int32, (32, 32), 0) == lax.broadcasted_iota(jnp.int32, (32, 32), 1)
        scale = jnp.sum(jnp.where(eye, gain[...], 0.0), axis=1, keepdims=True)

        def one(i, carry):
            ep, xp = i // NX, lax.rem(i, NX)
            at = pl.multiple_of(128 * xp, 128)
            a = mat[m, 2 * ep + el, :, pl.ds(at, 128)]
            b = mat[m, 2 * ep + el, :, pl.ds(pl.multiple_of(512 + at, 128), 128)]
            if m < 2:
                a, b = a * scale, b * scale
            xs[q, ep, 2 * xp] = jnp.where(low, a, pltpu.roll(b, 64, 1)).astype(BF)
            xs[q, ep, 2 * xp + 1] = jnp.where(low, pltpu.roll(a, 64, 1), b).astype(BF)
            return carry

        lax.fori_loop(0, 4 * NX, one, 0, unroll=4)

    def over_planes(q):
        send(xs.at[q, across, 0:4], fw.at[q, 0], a_send.at[q], f_recv.at[q, 0], {"tp": ahead})
        send(xs.at[q, across, 4:8], fw.at[q, 1], a_send.at[q], f_recv.at[q, 1], {"tp": behind})
        send(xs.at[q, ahead], ar.at[q, y], a_send.at[q], a_recv.at[q], {"tp": ahead})
        send(xs.at[q, behind], ar.at[q, y], a_send.at[q], a_recv.at[q], {"tp": behind})
        ar[q, y] = xs[q, y]

    def relay(q):
        wait_bytes(fw.at[q, 0], f_recv.at[q, 0])
        send(fw.at[q, 0], ar.at[q, behind, 0:4], f_send.at[q], a_recv.at[q], {"tp": ahead})
        wait_bytes(fw.at[q, 1], f_recv.at[q, 1])
        send(fw.at[q, 1], ar.at[q, ahead, 4:8], f_send.at[q], a_recv.at[q], {"tp": behind})

    def over_x(q):
        wait_bytes(ar.at[q, 0:3], a_recv.at[q])
        for off in range(1, NX * NC):
            j = lax.rem(me + off, NX * NC)
            send(
                ar.at[q, :, j], xr.at[q, me], x_send.at[q], x_recv.at[q],
                {"fs_1": j // 2, "fs_2": lax.rem(j, 2)},
            )
        xr[q, me] = ar[q, :, me]

    def over_z(q):
        wait_bytes(xr.at[q, 0:7], x_recv.at[q])

        def one(y0, carry):
            for half in range(2):
                rows = jnp.concatenate([xr[q, 4 * half + k, y0] for k in range(4)], axis=0)
                ts[q, y0, :, 128 * half : 128 * (half + 1)] = rows.T
            return carry

        lax.fori_loop(0, NY, one, 0)
        for off in (4, 3, 5, 2, 6, 1, 7):
            zp = lax.rem(z + off, NZ)
            rows = pl.multiple_of(64 * lax.rem(zp, 2), 64)
            send(
                ts.at[q, zp // 2, pl.ds(rows, 64), :], w.at[q, y, :, pl.ds(column, 256)],
                z_send.at[q], z_recv.at[q], {"fs_0": zp},
            )
        rows = pl.multiple_of(64 * lax.rem(z, 2), 64)
        w[q, y, :, pl.ds(column, 256)] = ts[q, z // 2, pl.ds(rows, 64), :]

    def spread(q):
        wait_bytes(w.at[q, 0, :, 0:1792], z_recv.at[q])
        send(w.at[q, y], w.at[q, y], c_send.at[q], c_recv.at[q, 0], {"tp": ahead})
        send(w.at[q, y], w.at[q, y], c_send.at[q], c_recv.at[q, 1], {"tp": behind})

    def spread_on(q):
        wait_bytes(w.at[q, behind], c_recv.at[q, 0])
        send(w.at[q, behind, 0:32], w.at[q, behind, 0:32], g_send.at[q], g_recv.at[q], {"tp": ahead})
        wait_bytes(w.at[q, ahead], c_recv.at[q, 1])
        send(w.at[q, ahead, 32:64], w.at[q, ahead, 32:64], g_send.at[q], g_recv.at[q], {"tp": behind})

    def arrived(q):
        wait_bytes(w.at[q, across], g_recv.at[q])
        m, el = CHUNKS[q]
        for ep in range(NY):
            pltpu.make_async_copy(w.at[q, ep], (og, ou)[m].at[2 * ep + el], o_sem.at[q]).start()

    def piece(p, plane):
        return w.at[4:6, plane, :, PIECE * p : PIECE * (p + 1)]

    def spread_down(p):
        if p == 0:
            for q in (4, 5):
                wait_bytes(w.at[q, 0, :, 0:1792], z_recv.at[q])
        send(piece(p, y), piece(p, y), c_send.at[4 + p], c_recv.at[4 + p, 0], {"tp": ahead})
        send(piece(p, y), piece(p, y), c_send.at[4 + p], c_recv.at[4 + p, 1], {"tp": behind})

    def spread_down_on(p):
        wait_bytes(piece(p, behind), c_recv.at[4 + p, 0])
        part = piece(p, behind).at[0]
        send(part, part, g_send.at[4 + p], g_recv.at[4 + p], {"tp": ahead})
        wait_bytes(piece(p, ahead), c_recv.at[4 + p, 1])
        part = piece(p, ahead).at[1]
        send(part, part, g_send.at[4 + p], g_recv.at[4 + p], {"tp": behind})

    def arrived_down(p):
        wait_bytes(piece(p, across), g_recv.at[4 + p])
        lanes = slice(PIECE * p, PIECE * (p + 1))
        for ep in range(NY):
            for el in range(2):
                pltpu.make_async_copy(
                    w.at[4 + el, ep, :, lanes], od.at[2 * ep + el, :, lanes], o_sem.at[4 + p]
                ).start()

    def normalize(i):
        if i == 0:
            reads[3].wait()
            expert = lax.broadcasted_iota(jnp.int32, (8, ROWS), 0)
            by_expert = jnp.where(ids[0:1, :] == expert, mix[0:1, :], 0.0)
            by_expert = by_expert + jnp.where(ids[1:2, :] == expert, mix[1:2, :], 0.0)
            gates[...] = by_expert.T

        def one(j, carry):
            rows = pl.ds(pl.multiple_of(64 * i + 16 * j, 16), 16)
            v = tok[rows, :].astype(F32)
            v = v - jnp.mean(v, axis=1, keepdims=True)
            var = jnp.mean(v * v, axis=1, keepdims=True)
            xn[rows, :] = (v * lax.rsqrt(var + norm_eps)).astype(BF)
            return carry

        lax.fori_loop(0, 4, one, 0, unroll=4)

    contract = (((1,), (1,)), ((), ()))

    def hide(el, i):
        rows = pl.ds(TILE * i, TILE)
        v = xn[rows, :]
        low = lax.broadcasted_iota(jnp.int32, (TILE, 128), 1) < 64
        first = 2 * el
        for pair in range(2):
            wg = w[first, 2 * pair : 2 * pair + 2].reshape(128, WIDTH)
            wu = w[first + 1, 2 * pair : 2 * pair + 2].reshape(128, WIDTH)
            g = lax.dot_general(v, wg, contract, preferred_element_type=F32)
            u = lax.dot_general(v, wu, contract, preferred_element_type=F32)
            e = 4 * pair + el
            share = jnp.where(low, gates[rows, e : e + 1], gates[rows, e + 2 : e + 3])
            h[rows, 256 * el + 128 * pair : 256 * el + 128 * (pair + 1)] = (
                g / (1.0 + jnp.exp(-g)) * u * share
            ).astype(BF)

    def part(rows, at):
        v = h[rows, :]
        a = w[4, :, :, pl.ds(at, BY_CORE)].reshape(256, BY_CORE)
        b = w[5, :, :, pl.ds(at, BY_CORE)].reshape(256, BY_CORE)
        return jnp.dot(v[:, 0:256], a, preferred_element_type=F32) + jnp.dot(
            v[:, 256:512], b, preferred_element_type=F32
        )

    def pair_of(k):
        return lax.rem(z // 2 + PAIRS[k], NP)

    def between_cores(s, k):
        i = NP * s + k
        rows = pl.ds(pl.multiple_of(2 * BLOCK * pair_of(k), 2 * BLOCK), 2 * BLOCK)
        pb[i] = part(rows, pl.multiple_of(LANES * s + BY_CORE * (1 - c), BY_CORE)).astype(BF)
        send(pb.at[i], r1.at[i], send1.at[i], recv1.at[i], {"fs_2": 1 - c})
        own[i] = part(rows, pl.multiple_of(LANES * s + BY_CORE * c, BY_CORE))

    def sum_x(s, k):
        i = NP * s + k
        wait_bytes(r1.at[i], recv1.at[i])
        total = (own[i] + r1[i].astype(F32)).astype(BF)
        for xp in range(NX):
            for half in range(2):
                s1[i, xp, half] = total[BLOCK * half : BLOCK * (half + 1), BY_X * xp : BY_X * (xp + 1)]
        send(s1.at[i, opposite, 0], t2.at[i, 0], sendt.at[i], recvt.at[i, 0], {"fs_1": right})
        send(s1.at[i, opposite, 1], t2.at[i, 1], sendt.at[i], recvt.at[i, 1], {"fs_1": left})
        send(s1.at[i, right, 1], r2.at[i, 1, 1], send2.at[i], recv2.at[i], {"fs_1": right})
        send(s1.at[i, left, 0], r2.at[i, 0, 1], send2.at[i], recv2.at[i], {"fs_1": left})

    def sum_x_on(s, k):
        i = NP * s + k
        wait_bytes(t2.at[i, 0], recvt.at[i, 0])
        u2[i, 0] = (s1[i, right, 0].astype(F32) + t2[i, 0].astype(F32)).astype(BF)
        send(u2.at[i, 0], r2.at[i, 0, 0], send2.at[i], recv2.at[i], {"fs_1": right})
        wait_bytes(t2.at[i, 1], recvt.at[i, 1])
        u2[i, 1] = (s1[i, left, 1].astype(F32) + t2[i, 1].astype(F32)).astype(BF)
        send(u2.at[i, 1], r2.at[i, 1, 0], send2.at[i], recv2.at[i], {"fs_1": left})

    def sum_z(s, k):
        i = NP * s + k
        wait_bytes(r2.at[i], recv2.at[i])
        for half in range(2):
            total = s1[i, x, half].astype(F32) + (r2[i, half, 0].astype(F32) + r2[i, half, 1].astype(F32))
            s2[i, half] = total.astype(BF)
        if PAIRS[k] == 0:
            here = lax.rem(z, 2)
            send(s2.at[i, 1 - here], r3.at[s, z], send3.at[i], recv3.at[s], {"fs_0": z + 1 - 2 * here})
            r3[s, z] = s2[i, here]
        else:
            for half in range(2):
                send(s2.at[i, half], r3.at[s, z], send3.at[i], recv3.at[s], {"fs_0": 2 * pair_of(k) + half})

    def give_rows(s):
        wait_bytes(r3.at[s, 0:7], recv3.at[s])
        total = r3[s, 0].astype(F32)
        for i in range(1, NZ):
            total = total + r3[s, i].astype(F32)
        row = lax.broadcasted_iota(jnp.int32, (128, BLOCK), 0)
        col = lax.broadcasted_iota(jnp.int32, (128, BLOCK), 1)
        within = lax.rem(row, 16)
        pick = ((col == (row // 16) * 12 + within) & (within < 12)).astype(BF)
        s4[s] = jnp.dot(pick, total.astype(BF), preferred_element_type=F32).astype(BF)
        at = pl.multiple_of(LANES * s + BY_CORE * c + BY_X * x, BY_X)
        for off in range(1, NX * NC):
            j = lax.rem(me + off, NX * NC)
            send(
                s4.at[s, pl.ds(pl.multiple_of(16 * j, 16), 16), :], r4.at[:, pl.ds(at, BY_X)],
                send4.at[s], recv4.at[s], {"fs_1": j // 2, "fs_2": lax.rem(j, 2)},
            )
        r4[:, pl.ds(at, BY_X)] = s4[s, pl.ds(pl.multiple_of(16 * me, 16), 16), :]

    for q in range(NQ):
        m, el = CHUNKS[q]
        if q in (0, 1, 4):
            reads[m].wait()
        pack(q)
    pl.semaphore_wait(barrier, len(peers))
    names = dict(
        A=over_planes, R=relay, X=over_x, Z=over_z, S=spread, F=spread_on, P=arrived, N=normalize, H=hide,
        T=spread_down, U=spread_down_on, V=arrived_down,
        B=between_cores, C=sum_x, D=sum_x_on, E=sum_z, G=give_rows,
    )
    for line in ORDER:
        for step in line.split():
            name, args = step[0], step[1:].split(",")
            names[name](*(int(a) for a in args))

    for q in range(NQ):
        wait_bytes(ar.at[q, 0:3], a_send.at[q])
        wait_bytes(fw.at[q], f_send.at[q])
        wait_bytes(xr.at[q, 0:7], x_send.at[q])
        wait_bytes(w.at[q, 0, :, 0:1792], z_send.at[q])
    for q in range(4):
        wait_bytes(w.at[q, 0:2], c_send.at[q])
        wait_bytes(w.at[q, 0], g_send.at[q])
        wait_bytes(w.at[q], o_sem.at[q])
    for p in range(PIECES):
        wait_bytes(w.at[4, :, :, 0:PIECE], c_send.at[4 + p])
        wait_bytes(piece(p, 0), g_send.at[4 + p])
        wait_bytes(w.at[4:6, :, :, 0:PIECE], o_sem.at[4 + p])
    for s in range(PASSES):
        for k in range(NP):
            i = NP * s + k
            wait_bytes(pb.at[i], send1.at[i])
            wait_bytes(t2.at[i], sendt.at[i])
            wait_bytes(r2.at[i], send2.at[i])
            if PAIRS[k] == 0:
                wait_bytes(s2.at[i, 0], send3.at[i])
            else:
                wait_bytes(s2.at[i], send3.at[i])
        wait_bytes(r4.at[:, 0 : 7 * BY_X], recv4.at[s])
    out[...] = r4[0:12, :]
    for s in range(PASSES):
        wait_bytes(r4.at[:, 0 : 7 * BY_X], send4.at[s])


def run(*args):
    weights = jax.ShapeDtypeStruct((8, 64, WIDTH), BF)
    vmem = pl.BlockSpec(memory_space=pltpu.VMEM)
    hbm = pl.BlockSpec(memory_space=pl.ANY)
    dma = pltpu.SemaphoreType.DMA
    return pl.pallas_call(
        kernel,
        out_shape=(weights, weights, weights, jax.ShapeDtypeStruct((12, WIDTH), BF)),
        in_specs=[hbm, vmem, vmem, vmem, hbm, hbm, hbm],
        out_specs=(hbm, hbm, hbm, vmem),
        scratch_shapes=[
            pltpu.VMEM((3, 8, 32, 1024), F32),
            pltpu.VMEM((ROWS, WIDTH), BF),
            pltpu.VMEM((NQ, NY, 8, 32, 128), BF),
            pltpu.VMEM((NQ, NY, 8, 32, 128), BF),
            pltpu.VMEM((NQ, 2, 4, 32, 128), BF),
            pltpu.VMEM((NQ, 8, NY, 32, 128), BF),
            pltpu.VMEM((NQ, NY, 128, 256), BF),
            pltpu.VMEM((NQ, NY, 64, WIDTH), BF),
            pltpu.VMEM((ROWS, WIDTH), BF),
            pltpu.VMEM((ROWS, 8), F32),
            pltpu.VMEM((ROWS, 512), BF),
            pltpu.VMEM((PASSES * NP, 2 * BLOCK, BY_CORE), BF),
            pltpu.VMEM((PASSES * NP, 2 * BLOCK, BY_CORE), F32),
            pltpu.VMEM((PASSES * NP, 2 * BLOCK, BY_CORE), BF),
            pltpu.VMEM((PASSES * NP, NX, 2, BLOCK, BY_X), BF),
            pltpu.VMEM((PASSES * NP, 2, BLOCK, BY_X), BF),
            pltpu.VMEM((PASSES * NP, 2, BLOCK, BY_X), BF),
            pltpu.VMEM((PASSES * NP, 2, 2, BLOCK, BY_X), BF),
            pltpu.VMEM((PASSES * NP, 2, BLOCK, BY_X), BF),
            pltpu.VMEM((PASSES, NZ, BLOCK, BY_X), BF),
            pltpu.VMEM((PASSES, 128, BY_X), BF),
            pltpu.VMEM((16, WIDTH), BF),
            dma((4,)),
            dma((NQ,)), dma((NQ,)),
            dma((NQ,)), dma((NQ, 2)),
            dma((NQ,)), dma((NQ,)),
            dma((NQ,)), dma((NQ,)),
            dma((4 + PIECES,)), dma((4 + PIECES, 2)),
            dma((4 + PIECES,)), dma((4 + PIECES,)),
            dma((4 + PIECES,)),
            dma((PASSES * NP,)), dma((PASSES * NP,)),
            dma((PASSES * NP,)), dma((PASSES * NP,)),
            dma((PASSES * NP,)), dma((PASSES * NP, 2)),
            dma((PASSES * NP,)), dma((PASSES,)),
            dma((PASSES,)), dma((PASSES,)),
        ],
        compiler_params=pltpu.CompilerParams(
            collective_id=0, has_side_effects=True, vmem_limit_bytes=60 * 1024 * 1024
        ),
        name="hand_over_and_serve",
    )(*args)


def put_kernel(wg, wu, wd, small, og, ou, od, out, buf, buf_small, sems):
    hops = [(small, buf_small, out)]
    for m, (w, o) in enumerate(((wg, og), (wu, ou), (wd, od))):
        for i in range(4):
            two = slice(2 * i, 2 * i + 2)
            hops.append((w.at[two], buf.at[m, two], o.at[two]))
    reads = [pltpu.make_async_copy(a, b, sems.at[0, n]) for n, (a, b, _) in enumerate(hops)]
    writes = [pltpu.make_async_copy(b, o, sems.at[1, n]) for n, (_, b, o) in enumerate(hops)]
    for copy in reads:
        copy.start()
    for read, write in zip(reads, writes):
        read.wait()
        write.start()
    for copy in writes:
        copy.wait()


def put_out(*results):
    weights = jax.ShapeDtypeStruct((8, 64, WIDTH), BF)
    small = jax.ShapeDtypeStruct((12, WIDTH), BF)
    hbm = pl.BlockSpec(memory_space=pl.ANY)
    return pl.pallas_call(
        put_kernel,
        out_shape=(weights, weights, weights, small),
        in_specs=[hbm] * 4,
        out_specs=(hbm, hbm, hbm, hbm),
        scratch_shapes=[
            pltpu.VMEM((3, 8, 64, WIDTH), BF),
            pltpu.VMEM((12, WIDTH), BF),
            pltpu.SemaphoreType.DMA((2, 13)),
        ],
        compiler_params=pltpu.CompilerParams(vmem_limit_bytes=60 * 1024 * 1024),
        name="put_out",
    )(*results)


def local(tokens, norm_gain, gate_weight, up_weight, down_weight, expert_ids, expert_mix):
    results = run(
        tokens.reshape(ROWS, WIDTH), expert_ids.reshape(ROWS, 2).T, expert_mix.reshape(ROWS, 2).T,
        norm_gain.reshape(1, 32), gate_weight, up_weight, down_weight,
    )
    gate_t, up_t, down_t, mixed = put_out(*results)
    turned = tuple(jnp.swapaxes(t, 1, 2) for t in (gate_t, up_t, down_t))
    return turned + (mixed.reshape(12, 1, WIDTH),)


def solution(mesh):
    finer = Mesh(mesh.devices.reshape(NZ, NX, NC, NY), ("fs_0", "fs_1", "fs_2", "tp"))
    placed = (
        P(None, "tp", None),
        P(FS),
        P(None, FS, "tp"),
        P(None, FS, "tp"),
        P(None, FS, "tp"),
        P(None, "tp", None),
        P(None, "tp", None),
    )
    return jax.shard_map(
        local,
        mesh=finer,
        in_specs=placed,
        out_specs=(P(None, None, FS), P(None, None, FS), P(None, None, FS), P(FS, "tp", None)),
        check_vma=False,
    )
```

```python
import jax
import jax.numpy as jnp
from jax import lax
from jax.experimental import pallas as pl
from jax.experimental.pallas import tpu as pltpu
from jax.sharding import Mesh
from jax.sharding import PartitionSpec as P

FS = ("fs_0", "fs_1", "fs_2")
NZ, NX, NC, NY = 8, 4, 2, 4
norm_eps = 1e-05
BF, F32 = jnp.bfloat16, jnp.float32
MESH = pl.DeviceIdType.MESH

CHUNKS = ((0, 0), (1, 0), (0, 1), (1, 1), (2, 0), (2, 1))
NQ = len(CHUNKS)
ROWS, WIDTH = 768, 2048
BLOCK = ROWS // NZ
EARLY = 2
PASSES = 4
PIECE = WIDTH // PASSES
BY_X = PIECE // NX
NP = 2
PART = ROWS // NC // NP
SHARE = BLOCK // NC
ORDER = (
    "A0 K1 A1 K2", "K3 K4 K5 R0", "A2 X0 R1 A3", "R2", "X1 A4 R3 X2", "Z0 A5 Q0,0 R4",
    "X3 Q0,1 Q0,7 Z1", "R5 Q1,0 X4 Q0,2", "Q0,6 X5 Z2 Q1,1", "Q1,7 Q0,3 Q0,5 N0",
    "Z3 Q1,2 Q1,6 N1", "Q0,4 Z4 N2 N3", "Q1,3 Q1,5 F0", "Z5 N4 N5",
    "Q1,4 N6 N7", "S2 N8 F1", "N9 N10 N11 P0",
    "S3 F2 P1", "H0,0 H0,1", "F3 T0 T1 P2", "P3 H1,0 H1,1",
    "U0 T2 U1 T3", "V0 B0,0 B0,1 U2", "C0,0 C0,1 V1 B1,0",
    "B1,1 U3 D0,0 C1,0", "D0,1 C1,1 V2", "B2,0 B2,1 E0,0 V3",
    "B3,0 B3,1 D1,0 E0,1", "C2,0 D1,1 C2,1 C3,0", "C3,1 E1,0 D2,0 G0",
    "E1,1 D2,1 D3,0 D3,1", "E2,0 G1 E2,1 E3,0", "E3,1 G2 G3",
)


def send(src, dst, send_sem, recv_sem, to):
    pltpu.make_async_remote_copy(
        src_ref=src, dst_ref=dst, send_sem=send_sem, recv_sem=recv_sem, device_id=to, device_id_type=MESH
    ).start()


def wait_bytes(ref, sem):
    pltpu.make_async_copy(ref, ref, sem).wait()


def kernel(
    tokens, ids_in, mix_in, gain_in, gate, up, down,
    og, ou, od, out,
    ids, mix, gain, mat, tok, xs, ar, fw, xr, ts, w, xn, gates, h,
    pb, own, r1, s1, t2, u2, r2, s2, r3, s4, r4,
    in_sem, a_send, a_recv, f_send, f_recv, x_send, x_recv, z_send, z_recv, n_recv,
    c_send, c_recv, g_send, g_recv, o_sem,
    send1, recv1, send2, recv2, sendt, recvt, send3, recv3, send4, recv4,
):
    z, x, c, y = (lax.axis_index(a) for a in ("fs_0", "fs_1", "fs_2", "tp"))
    me = 2 * x + c
    ahead, behind, across = (lax.rem(y + o, NY) for o in (1, 3, 2))
    right, left, opposite = (lax.rem(x + o, NX) for o in (1, 3, 2))
    column = pl.multiple_of(256 * z, 256)

    pairs = ((gain_in, gain), (gate, mat.at[0]), (up, mat.at[1]), (down, mat.at[2]), (tokens, tok), (ids_in, ids), (mix_in, mix))
    reads = [pltpu.make_async_copy(src, dst, in_sem.at[n]) for n, (src, dst) in enumerate(pairs)]
    for r in reads:
        r.start()

    barrier = pltpu.get_barrier_semaphore()
    peers = []
    for off in range(1, NX * NC):
        j = lax.rem(me + off, NX * NC)
        peers.append({"fs_1": j // 2, "fs_2": lax.rem(j, 2)})
    for off in range(1, NZ):
        peers.append({"fs_0": lax.rem(z + off, NZ)})
    peers += [{"tp": ahead}, {"tp": behind}]
    for to in peers:
        pl.semaphore_signal(barrier, inc=1, device_id=to, device_id_type=MESH)

    def pack(q):
        m, el = CHUNKS[q]
        if q == 0:
            reads[0].wait()
        if el == 0:
            reads[1 + m].wait()
        low = lax.broadcasted_iota(jnp.int32, (32, 128), 1) < 64
        eye = lax.broadcasted_iota(jnp.int32, (32, 32), 0) == lax.broadcasted_iota(jnp.int32, (32, 32), 1)
        scale = jnp.sum(jnp.where(eye, gain[...], 0.0), axis=1, keepdims=True)

        def one(i, carry):
            ep, xp = i // NX, lax.rem(i, NX)
            at = pl.multiple_of(128 * xp, 128)
            a = mat[m, 2 * ep + el, :, pl.ds(at, 128)]
            b = mat[m, 2 * ep + el, :, pl.ds(pl.multiple_of(512 + at, 128), 128)]
            if m < 2:
                a, b = a * scale, b * scale
            xs[q, ep, 2 * xp] = jnp.where(low, a, pltpu.roll(b, 64, 1)).astype(BF)
            xs[q, ep, 2 * xp + 1] = jnp.where(low, pltpu.roll(a, 64, 1), b).astype(BF)
            return carry

        lax.fori_loop(0, 4 * NX, one, 0, unroll=4)

    def over_planes(q):
        send(xs.at[q, across, 0:4], fw.at[q, 0], a_send.at[q], f_recv.at[q, 0], {"tp": ahead})
        send(xs.at[q, across, 4:8], fw.at[q, 1], a_send.at[q], f_recv.at[q, 1], {"tp": behind})
        send(xs.at[q, ahead], ar.at[q, y], a_send.at[q], a_recv.at[q], {"tp": ahead})
        send(xs.at[q, behind], ar.at[q, y], a_send.at[q], a_recv.at[q], {"tp": behind})
        ar[q, y] = xs[q, y]

    def relay(q):
        wait_bytes(fw.at[q, 0], f_recv.at[q, 0])
        send(fw.at[q, 0], ar.at[q, behind, 0:4], f_send.at[q], a_recv.at[q], {"tp": ahead})
        wait_bytes(fw.at[q, 1], f_recv.at[q, 1])
        send(fw.at[q, 1], ar.at[q, ahead, 4:8], f_send.at[q], a_recv.at[q], {"tp": behind})

    def over_x(q):
        wait_bytes(ar.at[q, 0:3], a_recv.at[q])
        for off in range(1, NX * NC):
            j = lax.rem(me + off, NX * NC)
            send(
                ar.at[q, :, j], xr.at[q, me], x_send.at[q], x_recv.at[q],
                {"fs_1": j // 2, "fs_2": lax.rem(j, 2)},
            )
        xr[q, me] = ar[q, :, me]

    def over_z(q):
        wait_bytes(xr.at[q, 0:7], x_recv.at[q])

        def one(y0, carry):
            for half in range(2):
                rows = jnp.concatenate([xr[q, 4 * half + k, y0] for k in range(4)], axis=0)
                ts[q, y0, :, 128 * half : 128 * (half + 1)] = rows.T
            return carry

        lax.fori_loop(0, NY, one, 0)
        for off in (1, 7, 2, 6, 3, 5, 4) if q < EARLY else (4, 3, 5, 2, 6, 1, 7):
            zp = lax.rem(z + off, NZ)
            rows = pl.multiple_of(64 * lax.rem(zp, 2), 64)
            send(
                ts.at[q, zp // 2, pl.ds(rows, 64), :], w.at[q, y, :, pl.ds(column, 256)],
                z_send.at[q], n_recv.at[q, off] if q < EARLY else z_recv.at[q], {"fs_0": zp},
            )
        rows = pl.multiple_of(64 * lax.rem(z, 2), 64)
        w[q, y, :, pl.ds(column, 256)] = ts[q, z // 2, pl.ds(rows, 64), :]

    def spread_first(q, off):
        lanes = pl.ds(pl.multiple_of(256 * lax.rem(z + NZ - off, NZ), 256), 256)
        if off > 0:
            wait_bytes(w.at[q, 0, :, 0:256], n_recv.at[q, off])
        block = w.at[q, y, :, lanes]
        send(block, block, c_send.at[q], c_recv.at[q, 0], {"tp": ahead})
        send(block, block, c_send.at[q], c_recv.at[q, 1], {"tp": behind})

    def spread(q):
        wait_bytes(w.at[q, 0, :, 0:1792], z_recv.at[q])
        send(w.at[q, y], w.at[q, y], c_send.at[q], c_recv.at[q, 0], {"tp": ahead})
        send(w.at[q, y], w.at[q, y], c_send.at[q], c_recv.at[q, 1], {"tp": behind})

    def spread_on(q):
        wait_bytes(w.at[q, behind], c_recv.at[q, 0])
        send(w.at[q, behind, 0:32], w.at[q, behind, 0:32], g_send.at[q], g_recv.at[q], {"tp": ahead})
        wait_bytes(w.at[q, ahead], c_recv.at[q, 1])
        send(w.at[q, ahead, 32:64], w.at[q, ahead, 32:64], g_send.at[q], g_recv.at[q], {"tp": behind})

    def arrived(q):
        wait_bytes(w.at[q, across], g_recv.at[q])
        m, el = CHUNKS[q]
        for ep in range(NY):
            pltpu.make_async_copy(w.at[q, ep], (og, ou)[m].at[2 * ep + el], o_sem.at[q]).start()

    def piece(p, plane):
        return w.at[4:6, plane, :, PIECE * p : PIECE * (p + 1)]

    def spread_down(p):
        if p == 0:
            for q in (4, 5):
                wait_bytes(w.at[q, 0, :, 0:1792], z_recv.at[q])
        send(piece(p, y), piece(p, y), c_send.at[4 + p], c_recv.at[4 + p, 0], {"tp": ahead})
        send(piece(p, y), piece(p, y), c_send.at[4 + p], c_recv.at[4 + p, 1], {"tp": behind})

    def spread_down_on(p):
        wait_bytes(piece(p, behind), c_recv.at[4 + p, 0])
        part = piece(p, behind).at[0]
        send(part, part, g_send.at[4 + p], g_recv.at[4 + p], {"tp": ahead})
        wait_bytes(piece(p, ahead), c_recv.at[4 + p, 1])
        part = piece(p, ahead).at[1]
        send(part, part, g_send.at[4 + p], g_recv.at[4 + p], {"tp": behind})

    def arrived_down(p):
        wait_bytes(piece(p, across), g_recv.at[4 + p])
        lanes = slice(PIECE * p, PIECE * (p + 1))
        for ep in range(NY):
            for el in range(2):
                pltpu.make_async_copy(
                    w.at[4 + el, ep, :, lanes], od.at[2 * ep + el, :, lanes], o_sem.at[4 + p]
                ).start()

    def normalize(i):
        if i == 0:
            for r in reads[4:]:
                r.wait()
            expert = lax.broadcasted_iota(jnp.int32, (8, ROWS), 0)
            by_expert = jnp.where(ids[0:1, :] == expert, mix[0:1, :], 0.0)
            by_expert = by_expert + jnp.where(ids[1:2, :] == expert, mix[1:2, :], 0.0)
            gates[...] = by_expert.T

        def one(j, carry):
            rows = pl.ds(pl.multiple_of(64 * i + 16 * j, 16), 16)
            v = tok[rows, :].astype(F32)
            v = v - jnp.mean(v, axis=1, keepdims=True)
            var = jnp.mean(v * v, axis=1, keepdims=True)
            xn[rows, :] = (v * lax.rsqrt(var + norm_eps)).astype(BF)
            return carry

        lax.fori_loop(0, 4, one, 0, unroll=4)

    contract = (((1,), (1,)), ((), ()))

    def hide(el, i):
        rows = pl.ds(NC * PART * i, NC * PART)
        v = xn[rows, :]
        low = lax.broadcasted_iota(jnp.int32, (NC * PART, 128), 1) < 64
        first = 2 * el
        for pair in range(2):
            wg = w[first, 2 * pair : 2 * pair + 2].reshape(128, WIDTH)
            wu = w[first + 1, 2 * pair : 2 * pair + 2].reshape(128, WIDTH)
            g = lax.dot_general(v, wg, contract, preferred_element_type=F32)
            u = lax.dot_general(v, wu, contract, preferred_element_type=F32)
            e = 4 * pair + el
            share = jnp.where(low, gates[rows, e : e + 1], gates[rows, e + 2 : e + 3])
            hid = (g / (1.0 + jnp.exp(-g)) * u * share).astype(BF)
            at = 256 * el + 128 * pair
            for b in range(NZ // NP):
                for core in range(NC):
                    h[core, PART * i + SHARE * b : PART * i + SHARE * (b + 1), at : at + 128] = hid[
                        BLOCK * b + SHARE * core : BLOCK * b + SHARE * (core + 1)
                    ]

    def side_of(k):
        return lax.rem(z // 4 + 1 - k, NP)

    def part(s, k, core):
        v = h[core, pl.ds(pl.multiple_of(PART * side_of(k), PART), PART), :]
        lanes = slice(PIECE * s, PIECE * (s + 1))
        a = w[4, :, :, lanes].reshape(256, PIECE)
        b = w[5, :, :, lanes].reshape(256, PIECE)
        return jnp.dot(v[:, 0:256], a, preferred_element_type=F32) + jnp.dot(
            v[:, 256:512], b, preferred_element_type=F32
        )

    def between_cores(s, k):
        i = NP * s + k
        pb[i] = part(s, k, 1 - c).astype(BF)
        send(pb.at[i], r1.at[i], send1.at[i], recv1.at[i], {"fs_2": 1 - c})
        own[i] = part(s, k, c)

    def sum_x(s, k):
        i = NP * s + k
        wait_bytes(r1.at[i], recv1.at[i])
        total = (own[i] + r1[i].astype(F32)).astype(BF)
        for xp in range(NX):
            for half in range(2):
                s1[i, xp, half] = total[BLOCK * half : BLOCK * (half + 1), BY_X * xp : BY_X * (xp + 1)]
        send(s1.at[i, opposite, 0], t2.at[i, 0], sendt.at[i], recvt.at[i, 0], {"fs_1": right})
        send(s1.at[i, opposite, 1], t2.at[i, 1], sendt.at[i], recvt.at[i, 1], {"fs_1": left})
        send(s1.at[i, right, 1], r2.at[i, 1, 1], send2.at[i], recv2.at[i], {"fs_1": right})
        send(s1.at[i, left, 0], r2.at[i, 0, 1], send2.at[i], recv2.at[i], {"fs_1": left})

    def sum_x_on(s, k):
        i = NP * s + k
        wait_bytes(t2.at[i, 0], recvt.at[i, 0])
        u2[i, 0] = (s1[i, right, 0].astype(F32) + t2[i, 0].astype(F32)).astype(BF)
        send(u2.at[i, 0], r2.at[i, 0, 0], send2.at[i], recv2.at[i], {"fs_1": right})
        wait_bytes(t2.at[i, 1], recvt.at[i, 1])
        u2[i, 1] = (s1[i, left, 1].astype(F32) + t2[i, 1].astype(F32)).astype(BF)
        send(u2.at[i, 1], r2.at[i, 1, 0], send2.at[i], recv2.at[i], {"fs_1": left})

    def sum_z(s, k):
        i = NP * s + k
        wait_bytes(r2.at[i], recv2.at[i])
        for half in range(2):
            total = s1[i, x, half].astype(F32) + (r2[i, half, 0].astype(F32) + r2[i, half, 1].astype(F32))
            for two in range(2):
                s2[i, 2 * half + two] = total[SHARE * two : SHARE * (two + 1)].astype(BF)
        here = lax.rem(z, 4)
        for step in range(k, 4):
            b = lax.rem(here + step, 4)
            send(s2.at[i, b], r3.at[s, z], send3.at[i], recv3.at[s], {"fs_0": 4 * side_of(k) + b})
        if k == 1:
            r3[s, z] = s2[i, here]

    amid = x // 2 == c

    def give_rows(s):
        wait_bytes(r3.at[s, 0:7], recv3.at[s])
        total = r3[s, 0].astype(F32)
        for i in range(1, NZ):
            total = total + r3[s, i].astype(F32)
        row = lax.broadcasted_iota(jnp.int32, (64, SHARE), 0)
        col = lax.broadcasted_iota(jnp.int32, (64, SHARE), 1)
        within = lax.rem(row, 16)
        pick = ((col == (row // 16) * 12 + within) & (within < 12)).astype(BF)
        got = jnp.dot(pick, total.astype(BF), preferred_element_type=F32).astype(BF)
        for i in range(4):
            s4[s, i] = got[16 * i : 16 * (i + 1)]
        lanes = pl.ds(pl.multiple_of(PIECE * s + BY_X * x, BY_X), BY_X)

        def give(i):
            j = 4 * c + i
            send(
                s4.at[s, i], r4.at[:, lanes], send4.at[s], recv4.at[s],
                {"fs_1": j // 2, "fs_2": lax.rem(j, 2)},
            )

        first = lax.rem(me, 4)
        for step in range(1, 4):
            give(lax.rem(first + step, 4))

        @pl.when(amid)
        def _():
            r4[:, lanes] = s4[s, first]

        @pl.when(jnp.logical_not(amid))
        def _():
            give(first)

    def wait_rows(s, sem):
        @pl.when(amid)
        def _():
            wait_bytes(r4.at[:, 0 : 3 * BY_X], sem.at[s])

        @pl.when(jnp.logical_not(amid))
        def _():
            wait_bytes(r4.at[:, 0 : 4 * BY_X], sem.at[s])

    pack(0)
    pl.semaphore_wait(barrier, len(peers))
    names = dict(
        K=pack, A=over_planes, R=relay, X=over_x, Z=over_z, Q=spread_first, S=spread, F=spread_on, P=arrived, N=normalize, H=hide,
        T=spread_down, U=spread_down_on, V=arrived_down,
        B=between_cores, C=sum_x, D=sum_x_on, E=sum_z, G=give_rows,
    )
    for line in ORDER:
        for step in line.split():
            name, args = step[0], step[1:].split(",")
            names[name](*(int(a) for a in args))

    for q in range(NQ):
        wait_bytes(ar.at[q, 0:3], a_send.at[q])
        wait_bytes(fw.at[q], f_send.at[q])
        wait_bytes(xr.at[q, 0:7], x_send.at[q])
        wait_bytes(w.at[q, 0, :, 0:1792], z_send.at[q])
    for q in range(4):
        wait_bytes(w.at[q, 0:2], c_send.at[q])
        wait_bytes(w.at[q, 0], g_send.at[q])
        wait_bytes(w.at[q], o_sem.at[q])
    for p in range(PASSES):
        wait_bytes(w.at[4, :, :, 0:PIECE], c_send.at[4 + p])
        wait_bytes(piece(p, 0), g_send.at[4 + p])
        wait_bytes(w.at[4:6, :, :, 0:PIECE], o_sem.at[4 + p])
    for s in range(PASSES):
        for k in range(NP):
            i = NP * s + k
            wait_bytes(pb.at[i], send1.at[i])
            wait_bytes(t2.at[i], sendt.at[i])
            wait_bytes(r2.at[i], send2.at[i])
            wait_bytes(s2.at[i, k:4], send3.at[i])
        wait_rows(s, recv4)
    out[...] = r4[0:12, :]
    for s in range(PASSES):
        wait_rows(s, send4)


def run(*args):
    weights = jax.ShapeDtypeStruct((8, 64, WIDTH), BF)
    vmem = pl.BlockSpec(memory_space=pltpu.VMEM)
    hbm = pl.BlockSpec(memory_space=pl.ANY)
    dma = pltpu.SemaphoreType.DMA
    return pl.pallas_call(
        kernel,
        out_shape=(weights, weights, weights, jax.ShapeDtypeStruct((12, WIDTH), BF)),
        in_specs=[hbm] * 7,
        out_specs=(hbm, hbm, hbm, vmem),
        scratch_shapes=[
            pltpu.VMEM((2, ROWS), jnp.int32),
            pltpu.VMEM((2, ROWS), F32),
            pltpu.VMEM((1, 32), F32),
            pltpu.VMEM((3, 8, 32, 1024), F32),
            pltpu.VMEM((ROWS, WIDTH), BF),
            pltpu.VMEM((NQ, NY, 8, 32, 128), BF),
            pltpu.VMEM((NQ, NY, 8, 32, 128), BF),
            pltpu.VMEM((NQ, 2, 4, 32, 128), BF),
            pltpu.VMEM((NQ, 8, NY, 32, 128), BF),
            pltpu.VMEM((NQ, NY, 128, 256), BF),
            pltpu.VMEM((NQ, NY, 64, WIDTH), BF),
            pltpu.VMEM((ROWS, WIDTH), BF),
            pltpu.VMEM((ROWS, 8), F32),
            pltpu.VMEM((NC, ROWS // NC, 512), BF),
            pltpu.VMEM((PASSES * NP, PART, PIECE), BF),
            pltpu.VMEM((PASSES * NP, PART, PIECE), F32),
            pltpu.VMEM((PASSES * NP, PART, PIECE), BF),
            pltpu.VMEM((PASSES * NP, NX, 2, BLOCK, BY_X), BF),
            pltpu.VMEM((PASSES * NP, 2, BLOCK, BY_X), BF),
            pltpu.VMEM((PASSES * NP, 2, BLOCK, BY_X), BF),
            pltpu.VMEM((PASSES * NP, 2, 2, BLOCK, BY_X), BF),
            pltpu.VMEM((PASSES * NP, 4, SHARE, BY_X), BF),
            pltpu.VMEM((PASSES, NZ, SHARE, BY_X), BF),
            pltpu.VMEM((PASSES, 4, 16, BY_X), BF),
            pltpu.VMEM((16, WIDTH), BF),
            dma((7,)),
            dma((NQ,)), dma((NQ,)),
            dma((NQ,)), dma((NQ, 2)),
            dma((NQ,)), dma((NQ,)),
            dma((NQ,)), dma((NQ,)), dma((EARLY, NZ)),
            dma((4 + PASSES,)), dma((4 + PASSES, 2)),
            dma((4 + PASSES,)), dma((4 + PASSES,)),
            dma((4 + PASSES,)),
            dma((PASSES * NP,)), dma((PASSES * NP,)),
            dma((PASSES * NP,)), dma((PASSES * NP,)),
            dma((PASSES * NP,)), dma((PASSES * NP, 2)),
            dma((PASSES * NP,)), dma((PASSES,)),
            dma((PASSES,)), dma((PASSES,)),
        ],
        compiler_params=pltpu.CompilerParams(
            collective_id=0, has_side_effects=True, vmem_limit_bytes=60 * 1024 * 1024
        ),
        name="hand_over_and_serve",
    )(*args)


def put_kernel(wg, wu, wd, small, og, ou, od, out, buf, buf_small, sems):
    hops = [(small, buf_small, out)]
    for m, (w, o) in enumerate(((wg, og), (wu, ou), (wd, od))):
        for i in range(4):
            two = slice(2 * i, 2 * i + 2)
            hops.append((w.at[two], buf.at[m, two], o.at[two]))
    reads = [pltpu.make_async_copy(a, b, sems.at[0, n]) for n, (a, b, _) in enumerate(hops)]
    writes = [pltpu.make_async_copy(b, o, sems.at[1, n]) for n, (_, b, o) in enumerate(hops)]
    for copy in reads:
        copy.start()
    for read, write in zip(reads, writes):
        read.wait()
        write.start()
    for copy in writes:
        copy.wait()


def put_out(*results):
    weights = jax.ShapeDtypeStruct((8, 64, WIDTH), BF)
    small = jax.ShapeDtypeStruct((12, WIDTH), BF)
    hbm = pl.BlockSpec(memory_space=pl.ANY)
    return pl.pallas_call(
        put_kernel,
        out_shape=(weights, weights, weights, small),
        in_specs=[hbm] * 4,
        out_specs=(hbm, hbm, hbm, hbm),
        scratch_shapes=[
            pltpu.VMEM((3, 8, 64, WIDTH), BF),
            pltpu.VMEM((12, WIDTH), BF),
            pltpu.SemaphoreType.DMA((2, 13)),
        ],
        compiler_params=pltpu.CompilerParams(vmem_limit_bytes=60 * 1024 * 1024),
        name="put_out",
    )(*results)


def local(tokens, norm_gain, gate_weight, up_weight, down_weight, expert_ids, expert_mix):
    results = run(
        tokens.reshape(ROWS, WIDTH), expert_ids.reshape(ROWS, 2).T, expert_mix.reshape(ROWS, 2).T,
        norm_gain.reshape(1, 32), gate_weight, up_weight, down_weight,
    )
    gate_t, up_t, down_t, mixed = put_out(*results)
    turned = tuple(jnp.swapaxes(t, 1, 2) for t in (gate_t, up_t, down_t))
    return turned + (mixed.reshape(12, 1, WIDTH),)


def solution(mesh):
    finer = Mesh(mesh.devices.reshape(NZ, NX, NC, NY), ("fs_0", "fs_1", "fs_2", "tp"))
    placed = (
        P(None, "tp", None),
        P(FS),
        P(None, FS, "tp"),
        P(None, FS, "tp"),
        P(None, FS, "tp"),
        P(None, "tp", None),
        P(None, "tp", None),
    )
    return jax.shard_map(
        local,
        mesh=finer,
        in_specs=placed,
        out_specs=(P(None, None, FS), P(None, None, FS), P(None, None, FS), P(FS, "tp", None)),
        check_vma=False,
    )
```

```python
import jax
import jax.numpy as jnp
from jax import lax
from jax.experimental import pallas as pl
from jax.experimental.pallas import tpu as pltpu
from jax.sharding import Mesh
from jax.sharding import PartitionSpec as P

FS = ("fs_0", "fs_1", "fs_2")
NZ, NX, NC, NY = 8, 4, 2, 4
norm_eps = 1e-05
BF, F32 = jnp.bfloat16, jnp.float32
MESH = pl.DeviceIdType.MESH

CHUNKS = ((0, 0), (1, 0), (0, 1), (1, 1), (2, 0), (2, 1))
NQ = len(CHUNKS)
ROWS, WIDTH = 768, 2048
BLOCK = ROWS // NZ
EARLY = 3
PASSES = 4
PIECE = WIDTH // PASSES
BY_X = PIECE // NX
NP = 2
PART = ROWS // NC // NP
SHARE = BLOCK // NC
ORDER = (
    "A0 K1 K2 K3", "R0 A1 K4 K5", "A2 X0 R1 A3", "R2", "X1 A4 R3 X2", "Z0 A5 Q0,0 R4",
    "X3 Q0,1 Q0,7 Z1", "R5 Q1,0 X4 Q0,2", "Q0,6 X5 Z2 Q1,1", "Q1,7 Q0,3 Q0,5 N0",
    "Z3 Q1,2 Q1,6 N1", "Q0,4 Z4 N2 N3", "Q1,3 Q1,5 F0", "Z5 Q2,0 N4 N5",
    "Q1,4 Q2,1 Q2,7 N6", "Q2,2 Q2,6 N7 N8", "Q2,3 Q2,5 N9 N10", "F1 Q2,4 N11 P0",
    "S3 F2 P1", "H0,0 H0,1", "F3 T0 T1 P2", "P3 H1,0 U0 T2",
    "H1,1 U1 T3", "V0 B0,0 B0,1 U2", "C0,0 C0,1 V1 B1,0",
    "B1,1 U3 D0,0 C1,0", "D0,1 C1,1 V2", "B2,0 B2,1 E0,0 V3",
    "B3,0 B3,1 D1,0 E0,1", "C2,0 D1,1 C2,1 C3,0", "C3,1 E1,0 D2,0 G0",
    "E1,1 D2,1 D3,0 D3,1", "E2,0 G1 E2,1 E3,0", "E3,1 G2 G3",
)


def send(src, dst, send_sem, recv_sem, to):
    pltpu.make_async_remote_copy(
        src_ref=src, dst_ref=dst, send_sem=send_sem, recv_sem=recv_sem, device_id=to, device_id_type=MESH
    ).start()


def wait_bytes(ref, sem):
    pltpu.make_async_copy(ref, ref, sem).wait()


def kernel(
    tokens, ids_in, mix_in, gain_in, gate, up, down,
    og, ou, od, out,
    ids, mix, gain, mat, tok, xs, ar, fw, xr, ts, w, xn, gates, h,
    pb, own, r1, s1, t2, u2, r2, s2, r3, s4, r4,
    in_sem, a_send, a_recv, f_send, f_recv, x_send, x_recv, z_send, z_recv, n_recv,
    c_send, c_recv, g_send, g_recv, o_sem,
    send1, recv1, send2, recv2, sendt, recvt, send3, recv3, send4, recv4,
):
    z, x, c, y = (lax.axis_index(a) for a in ("fs_0", "fs_1", "fs_2", "tp"))
    me = 2 * x + c
    ahead, behind, across = (lax.rem(y + o, NY) for o in (1, 3, 2))
    right, left, opposite = (lax.rem(x + o, NX) for o in (1, 3, 2))
    column = pl.multiple_of(256 * z, 256)

    pairs = ((gain_in, gain), (gate, mat.at[0]), (up, mat.at[1]), (down, mat.at[2]), (tokens, tok), (ids_in, ids), (mix_in, mix))
    reads = [pltpu.make_async_copy(src, dst, in_sem.at[n]) for n, (src, dst) in enumerate(pairs)]
    for r in reads:
        r.start()

    barrier = pltpu.get_barrier_semaphore()
    peers = []
    for off in range(1, NX * NC):
        j = lax.rem(me + off, NX * NC)
        peers.append({"fs_1": j // 2, "fs_2": lax.rem(j, 2)})
    for off in range(1, NZ):
        peers.append({"fs_0": lax.rem(z + off, NZ)})
    peers += [{"tp": ahead}, {"tp": behind}]
    for to in peers:
        pl.semaphore_signal(barrier, inc=1, device_id=to, device_id_type=MESH)

    def pack(q):
        m, el = CHUNKS[q]
        if q == 0:
            reads[0].wait()
        if el == 0:
            reads[1 + m].wait()
        low = lax.broadcasted_iota(jnp.int32, (32, 128), 1) < 64
        eye = lax.broadcasted_iota(jnp.int32, (32, 32), 0) == lax.broadcasted_iota(jnp.int32, (32, 32), 1)
        scale = jnp.sum(jnp.where(eye, gain[...], 0.0), axis=1, keepdims=True)

        def one(i, carry):
            ep, xp = i // NX, lax.rem(i, NX)
            at = pl.multiple_of(128 * xp, 128)
            a = mat[m, 2 * ep + el, :, pl.ds(at, 128)]
            b = mat[m, 2 * ep + el, :, pl.ds(pl.multiple_of(512 + at, 128), 128)]
            if m < 2:
                a, b = a * scale, b * scale
            xs[q, ep, 2 * xp] = jnp.where(low, a, pltpu.roll(b, 64, 1)).astype(BF)
            xs[q, ep, 2 * xp + 1] = jnp.where(low, pltpu.roll(a, 64, 1), b).astype(BF)
            return carry

        lax.fori_loop(0, 4 * NX, one, 0, unroll=4)

    def over_planes(q):
        send(xs.at[q, across, 0:4], fw.at[q, 0], a_send.at[q], f_recv.at[q, 0], {"tp": ahead})
        send(xs.at[q, across, 4:8], fw.at[q, 1], a_send.at[q], f_recv.at[q, 1], {"tp": behind})
        send(xs.at[q, ahead], ar.at[q, y], a_send.at[q], a_recv.at[q], {"tp": ahead})
        send(xs.at[q, behind], ar.at[q, y], a_send.at[q], a_recv.at[q], {"tp": behind})
        ar[q, y] = xs[q, y]

    def relay(q):
        wait_bytes(fw.at[q, 0], f_recv.at[q, 0])
        send(fw.at[q, 0], ar.at[q, behind, 0:4], f_send.at[q], a_recv.at[q], {"tp": ahead})
        wait_bytes(fw.at[q, 1], f_recv.at[q, 1])
        send(fw.at[q, 1], ar.at[q, ahead, 4:8], f_send.at[q], a_recv.at[q], {"tp": behind})

    def over_x(q):
        wait_bytes(ar.at[q, 0:3], a_recv.at[q])
        for off in range(1, NX * NC):
            j = lax.rem(me + off, NX * NC)
            send(
                ar.at[q, :, j], xr.at[q, me], x_send.at[q], x_recv.at[q],
                {"fs_1": j // 2, "fs_2": lax.rem(j, 2)},
            )
        xr[q, me] = ar[q, :, me]

    def over_z(q):
        wait_bytes(xr.at[q, 0:7], x_recv.at[q])

        def one(y0, carry):
            for half in range(2):
                rows = jnp.concatenate([xr[q, 4 * half + k, y0] for k in range(4)], axis=0)
                ts[q, y0, :, 128 * half : 128 * (half + 1)] = rows.T
            return carry

        lax.fori_loop(0, NY, one, 0)
        for off in (1, 7, 2, 6, 3, 5, 4) if q < EARLY else (4, 3, 5, 2, 6, 1, 7):
            zp = lax.rem(z + off, NZ)
            rows = pl.multiple_of(64 * lax.rem(zp, 2), 64)
            send(
                ts.at[q, zp // 2, pl.ds(rows, 64), :], w.at[q, y, :, pl.ds(column, 256)],
                z_send.at[q], n_recv.at[q, off] if q < EARLY else z_recv.at[q], {"fs_0": zp},
            )
        rows = pl.multiple_of(64 * lax.rem(z, 2), 64)
        w[q, y, :, pl.ds(column, 256)] = ts[q, z // 2, pl.ds(rows, 64), :]

    def spread_first(q, off):
        lanes = pl.ds(pl.multiple_of(256 * lax.rem(z + NZ - off, NZ), 256), 256)
        if off > 0:
            wait_bytes(w.at[q, 0, :, 0:256], n_recv.at[q, off])
        block = w.at[q, y, :, lanes]
        send(block, block, c_send.at[q], c_recv.at[q, 0], {"tp": ahead})
        send(block, block, c_send.at[q], c_recv.at[q, 1], {"tp": behind})

    def spread(q):
        wait_bytes(w.at[q, 0, :, 0:1792], z_recv.at[q])
        send(w.at[q, y], w.at[q, y], c_send.at[q], c_recv.at[q, 0], {"tp": ahead})
        send(w.at[q, y], w.at[q, y], c_send.at[q], c_recv.at[q, 1], {"tp": behind})

    def spread_on(q):
        wait_bytes(w.at[q, behind], c_recv.at[q, 0])
        send(w.at[q, behind, 0:32], w.at[q, behind, 0:32], g_send.at[q], g_recv.at[q], {"tp": ahead})
        wait_bytes(w.at[q, ahead], c_recv.at[q, 1])
        send(w.at[q, ahead, 32:64], w.at[q, ahead, 32:64], g_send.at[q], g_recv.at[q], {"tp": behind})

    def arrived(q):
        wait_bytes(w.at[q, across], g_recv.at[q])
        m, el = CHUNKS[q]
        for ep in range(NY):
            pltpu.make_async_copy(w.at[q, ep], (og, ou)[m].at[2 * ep + el], o_sem.at[q]).start()

    def piece(p, plane):
        return w.at[4:6, plane, :, PIECE * p : PIECE * (p + 1)]

    def spread_down(p):
        if p == 0:
            for q in (4, 5):
                wait_bytes(w.at[q, 0, :, 0:1792], z_recv.at[q])
        send(piece(p, y), piece(p, y), c_send.at[4 + p], c_recv.at[4 + p, 0], {"tp": ahead})
        send(piece(p, y), piece(p, y), c_send.at[4 + p], c_recv.at[4 + p, 1], {"tp": behind})

    def spread_down_on(p):
        wait_bytes(piece(p, behind), c_recv.at[4 + p, 0])
        part = piece(p, behind).at[0]
        send(part, part, g_send.at[4 + p], g_recv.at[4 + p], {"tp": ahead})
        wait_bytes(piece(p, ahead), c_recv.at[4 + p, 1])
        part = piece(p, ahead).at[1]
        send(part, part, g_send.at[4 + p], g_recv.at[4 + p], {"tp": behind})

    def arrived_down(p):
        wait_bytes(piece(p, across), g_recv.at[4 + p])
        lanes = slice(PIECE * p, PIECE * (p + 1))
        for ep in range(NY):
            for el in range(2):
                pltpu.make_async_copy(
                    w.at[4 + el, ep, :, lanes], od.at[2 * ep + el, :, lanes], o_sem.at[4 + p]
                ).start()

    def normalize(i):
        if i == 0:
            for r in reads[4:]:
                r.wait()
            expert = lax.broadcasted_iota(jnp.int32, (8, ROWS), 0)
            by_expert = jnp.where(ids[0:1, :] == expert, mix[0:1, :], 0.0)
            by_expert = by_expert + jnp.where(ids[1:2, :] == expert, mix[1:2, :], 0.0)
            gates[...] = by_expert.T

        def one(j, carry):
            rows = pl.ds(pl.multiple_of(64 * i + 16 * j, 16), 16)
            v = tok[rows, :].astype(F32)
            v = v - jnp.mean(v, axis=1, keepdims=True)
            var = jnp.mean(v * v, axis=1, keepdims=True)
            xn[rows, :] = (v * lax.rsqrt(var + norm_eps)).astype(BF)
            return carry

        lax.fori_loop(0, 4, one, 0, unroll=4)

    contract = (((1,), (1,)), ((), ()))

    def hide(el, i):
        rows = pl.ds(NC * PART * i, NC * PART)
        v = xn[rows, :]
        low = lax.broadcasted_iota(jnp.int32, (NC * PART, 128), 1) < 64
        first = 2 * el
        for pair in range(2):
            wg = w[first, 2 * pair : 2 * pair + 2].reshape(128, WIDTH)
            wu = w[first + 1, 2 * pair : 2 * pair + 2].reshape(128, WIDTH)
            g = lax.dot_general(v, wg, contract, preferred_element_type=F32)
            u = lax.dot_general(v, wu, contract, preferred_element_type=F32)
            e = 4 * pair + el
            share = jnp.where(low, gates[rows, e : e + 1], gates[rows, e + 2 : e + 3])
            hid = (g / (1.0 + jnp.exp(-g)) * u * share).astype(BF)
            at = 256 * el + 128 * pair
            for b in range(NZ // NP):
                for core in range(NC):
                    h[core, PART * i + SHARE * b : PART * i + SHARE * (b + 1), at : at + 128] = hid[
                        BLOCK * b + SHARE * core : BLOCK * b + SHARE * (core + 1)
                    ]

    def side_of(k):
        return lax.rem(z // 4 + 1 - k, NP)

    def part(s, k, core):
        v = h[core, pl.ds(pl.multiple_of(PART * side_of(k), PART), PART), :]
        lanes = slice(PIECE * s, PIECE * (s + 1))
        a = w[4, :, :, lanes].reshape(256, PIECE)
        b = w[5, :, :, lanes].reshape(256, PIECE)
        return jnp.dot(v[:, 0:256], a, preferred_element_type=F32) + jnp.dot(
            v[:, 256:512], b, preferred_element_type=F32
        )

    def between_cores(s, k):
        i = NP * s + k
        pb[i] = part(s, k, 1 - c).astype(BF)
        send(pb.at[i], r1.at[i], send1.at[i], recv1.at[i], {"fs_2": 1 - c})
        own[i] = part(s, k, c)

    def sum_x(s, k):
        i = NP * s + k
        wait_bytes(r1.at[i], recv1.at[i])
        total = (own[i] + r1[i].astype(F32)).astype(BF)
        for xp in range(NX):
            for half in range(2):
                s1[i, xp, half] = total[BLOCK * half : BLOCK * (half + 1), BY_X * xp : BY_X * (xp + 1)]
        send(s1.at[i, opposite, 0], t2.at[i, 0], sendt.at[i], recvt.at[i, 0], {"fs_1": right})
        send(s1.at[i, opposite, 1], t2.at[i, 1], sendt.at[i], recvt.at[i, 1], {"fs_1": left})
        send(s1.at[i, right, 1], r2.at[i, 1, 1], send2.at[i], recv2.at[i], {"fs_1": right})
        send(s1.at[i, left, 0], r2.at[i, 0, 1], send2.at[i], recv2.at[i], {"fs_1": left})

    def sum_x_on(s, k):
        i = NP * s + k
        wait_bytes(t2.at[i, 0], recvt.at[i, 0])
        u2[i, 0] = (s1[i, right, 0].astype(F32) + t2[i, 0].astype(F32)).astype(BF)
        send(u2.at[i, 0], r2.at[i, 0, 0], send2.at[i], recv2.at[i], {"fs_1": right})
        wait_bytes(t2.at[i, 1], recvt.at[i, 1])
        u2[i, 1] = (s1[i, left, 1].astype(F32) + t2[i, 1].astype(F32)).astype(BF)
        send(u2.at[i, 1], r2.at[i, 1, 0], send2.at[i], recv2.at[i], {"fs_1": left})

    def sum_z(s, k):
        i = NP * s + k
        wait_bytes(r2.at[i], recv2.at[i])
        for half in range(2):
            total = s1[i, x, half].astype(F32) + (r2[i, half, 0].astype(F32) + r2[i, half, 1].astype(F32))
            for two in range(2):
                s2[i, 2 * half + two] = total[SHARE * two : SHARE * (two + 1)].astype(BF)
        here = lax.rem(z, 4)
        for step in range(k, 4):
            b = lax.rem(here + step, 4)
            send(s2.at[i, b], r3.at[s, z], send3.at[i], recv3.at[s], {"fs_0": 4 * side_of(k) + b})
        if k == 1:
            r3[s, z] = s2[i, here]

    amid = x // 2 == c

    def give_rows(s):
        wait_bytes(r3.at[s, 0:7], recv3.at[s])
        total = r3[s, 0].astype(F32)
        for i in range(1, NZ):
            total = total + r3[s, i].astype(F32)
        row = lax.broadcasted_iota(jnp.int32, (64, SHARE), 0)
        col = lax.broadcasted_iota(jnp.int32, (64, SHARE), 1)
        within = lax.rem(row, 16)
        pick = ((col == (row // 16) * 12 + within) & (within < 12)).astype(BF)
        got = jnp.dot(pick, total.astype(BF), preferred_element_type=F32).astype(BF)
        for i in range(4):
            s4[s, i] = got[16 * i : 16 * (i + 1)]
        lanes = pl.ds(pl.multiple_of(PIECE * s + BY_X * x, BY_X), BY_X)

        def give(i):
            j = 4 * c + i
            send(
                s4.at[s, i], r4.at[:, lanes], send4.at[s], recv4.at[s],
                {"fs_1": j // 2, "fs_2": lax.rem(j, 2)},
            )

        first = lax.rem(me, 4)
        for step in range(1, 4):
            give(lax.rem(first + step, 4))

        @pl.when(amid)
        def _():
            r4[:, lanes] = s4[s, first]

        @pl.when(jnp.logical_not(amid))
        def _():
            give(first)

    def wait_rows(s, sem):
        @pl.when(amid)
        def _():
            wait_bytes(r4.at[:, 0 : 3 * BY_X], sem.at[s])

        @pl.when(jnp.logical_not(amid))
        def _():
            wait_bytes(r4.at[:, 0 : 4 * BY_X], sem.at[s])

    pack(0)
    pl.semaphore_wait(barrier, len(peers))
    names = dict(
        K=pack, A=over_planes, R=relay, X=over_x, Z=over_z, Q=spread_first, S=spread, F=spread_on, P=arrived, N=normalize, H=hide,
        T=spread_down, U=spread_down_on, V=arrived_down,
        B=between_cores, C=sum_x, D=sum_x_on, E=sum_z, G=give_rows,
    )
    for line in ORDER:
        for step in line.split():
            name, args = step[0], step[1:].split(",")
            names[name](*(int(a) for a in args))

    for q in range(NQ):
        wait_bytes(ar.at[q, 0:3], a_send.at[q])
        wait_bytes(fw.at[q], f_send.at[q])
        wait_bytes(xr.at[q, 0:7], x_send.at[q])
        wait_bytes(w.at[q, 0, :, 0:1792], z_send.at[q])
    for q in range(4):
        wait_bytes(w.at[q, 0:2], c_send.at[q])
        wait_bytes(w.at[q, 0], g_send.at[q])
        wait_bytes(w.at[q], o_sem.at[q])
    for p in range(PASSES):
        wait_bytes(w.at[4, :, :, 0:PIECE], c_send.at[4 + p])
        wait_bytes(piece(p, 0), g_send.at[4 + p])
        wait_bytes(w.at[4:6, :, :, 0:PIECE], o_sem.at[4 + p])
    for s in range(PASSES):
        for k in range(NP):
            i = NP * s + k
            wait_bytes(pb.at[i], send1.at[i])
            wait_bytes(t2.at[i], sendt.at[i])
            wait_bytes(r2.at[i], send2.at[i])
            wait_bytes(s2.at[i, k:4], send3.at[i])
        wait_rows(s, recv4)
    out[...] = r4[0:12, :]
    for s in range(PASSES):
        wait_rows(s, send4)


def run(*args):
    weights = jax.ShapeDtypeStruct((8, 64, WIDTH), BF)
    vmem = pl.BlockSpec(memory_space=pltpu.VMEM)
    hbm = pl.BlockSpec(memory_space=pl.ANY)
    dma = pltpu.SemaphoreType.DMA
    return pl.pallas_call(
        kernel,
        out_shape=(weights, weights, weights, jax.ShapeDtypeStruct((12, WIDTH), BF)),
        in_specs=[hbm] * 7,
        out_specs=(hbm, hbm, hbm, vmem),
        scratch_shapes=[
            pltpu.VMEM((2, ROWS), jnp.int32),
            pltpu.VMEM((2, ROWS), F32),
            pltpu.VMEM((1, 32), F32),
            pltpu.VMEM((3, 8, 32, 1024), F32),
            pltpu.VMEM((ROWS, WIDTH), BF),
            pltpu.VMEM((NQ, NY, 8, 32, 128), BF),
            pltpu.VMEM((NQ, NY, 8, 32, 128), BF),
            pltpu.VMEM((NQ, 2, 4, 32, 128), BF),
            pltpu.VMEM((NQ, 8, NY, 32, 128), BF),
            pltpu.VMEM((NQ, NY, 128, 256), BF),
            pltpu.VMEM((NQ, NY, 64, WIDTH), BF),
            pltpu.VMEM((ROWS, WIDTH), BF),
            pltpu.VMEM((ROWS, 8), F32),
            pltpu.VMEM((NC, ROWS // NC, 512), BF),
            pltpu.VMEM((PASSES * NP, PART, PIECE), BF),
            pltpu.VMEM((PASSES * NP, PART, PIECE), F32),
            pltpu.VMEM((PASSES * NP, PART, PIECE), BF),
            pltpu.VMEM((PASSES * NP, NX, 2, BLOCK, BY_X), BF),
            pltpu.VMEM((PASSES * NP, 2, BLOCK, BY_X), BF),
            pltpu.VMEM((PASSES * NP, 2, BLOCK, BY_X), BF),
            pltpu.VMEM((PASSES * NP, 2, 2, BLOCK, BY_X), BF),
            pltpu.VMEM((PASSES * NP, 4, SHARE, BY_X), BF),
            pltpu.VMEM((PASSES, NZ, SHARE, BY_X), BF),
            pltpu.VMEM((PASSES, 4, 16, BY_X), BF),
            pltpu.VMEM((16, WIDTH), BF),
            dma((7,)),
            dma((NQ,)), dma((NQ,)),
            dma((NQ,)), dma((NQ, 2)),
            dma((NQ,)), dma((NQ,)),
            dma((NQ,)), dma((NQ,)), dma((EARLY, NZ)),
            dma((4 + PASSES,)), dma((4 + PASSES, 2)),
            dma((4 + PASSES,)), dma((4 + PASSES,)),
            dma((4 + PASSES,)),
            dma((PASSES * NP,)), dma((PASSES * NP,)),
            dma((PASSES * NP,)), dma((PASSES * NP,)),
            dma((PASSES * NP,)), dma((PASSES * NP, 2)),
            dma((PASSES * NP,)), dma((PASSES,)),
            dma((PASSES,)), dma((PASSES,)),
        ],
        compiler_params=pltpu.CompilerParams(
            collective_id=0, has_side_effects=True, vmem_limit_bytes=40 * 1024 * 1024
        ),
        name="hand_over_and_serve",
    )(*args)


def put_kernel(wg, wu, wd, small, og, ou, od, out, sems):
    hops = [(small, out)]
    for w, o in ((wg, og), (wu, ou), (wd, od)):
        for i in range(4):
            two = slice(2 * i, 2 * i + 2)
            hops.append((w.at[two], o.at[two]))
    writes = [pltpu.make_async_copy(a, o, sems.at[n]) for n, (a, o) in enumerate(hops)]
    for copy in writes:
        copy.start()
    for copy in writes:
        copy.wait()


def put_out(*results):
    weights = jax.ShapeDtypeStruct((8, 64, WIDTH), BF)
    small = jax.ShapeDtypeStruct((12, WIDTH), BF)
    hbm = pl.BlockSpec(memory_space=pl.ANY)
    vmem = pl.BlockSpec(memory_space=pltpu.VMEM)
    return pl.pallas_call(
        put_kernel,
        out_shape=(weights, weights, weights, small),
        in_specs=[vmem] * 4,
        out_specs=(hbm, hbm, hbm, hbm),
        scratch_shapes=[pltpu.SemaphoreType.DMA((13,))],
        compiler_params=pltpu.CompilerParams(vmem_limit_bytes=16 * 1024 * 1024),
        name="put_out",
    )(*results)


def local(tokens, norm_gain, gate_weight, up_weight, down_weight, expert_ids, expert_mix):
    args = (
        tokens.reshape(ROWS, WIDTH), expert_ids.reshape(ROWS, 2).T, expert_mix.reshape(ROWS, 2).T,
        norm_gain.reshape(1, 32), gate_weight, up_weight, down_weight,
    )
    results = run(*(pltpu.with_memory_space_constraint(a, pltpu.HBM) for a in args))
    gate_t, up_t, down_t, mixed = put_out(*results)
    turned = tuple(jnp.swapaxes(t, 1, 2) for t in (gate_t, up_t, down_t))
    return turned + (mixed.reshape(12, 1, WIDTH),)


def solution(mesh):
    finer = Mesh(mesh.devices.reshape(NZ, NX, NC, NY), ("fs_0", "fs_1", "fs_2", "tp"))
    placed = (
        P(None, "tp", None),
        P(FS),
        P(None, FS, "tp"),
        P(None, FS, "tp"),
        P(None, FS, "tp"),
        P(None, "tp", None),
        P(None, "tp", None),
    )
    return jax.shard_map(
        local,
        mesh=finer,
        in_specs=placed,
        out_specs=(P(None, None, FS), P(None, None, FS), P(None, None, FS), P(FS, "tp", None)),
        check_vma=False,
    )
```

```python
import jax
import jax.numpy as jnp
from jax import lax
from jax.experimental import pallas as pl
from jax.experimental.pallas import tpu as pltpu
from jax.sharding import Mesh
from jax.sharding import PartitionSpec as P

FS = ("fs_0", "fs_1", "fs_2")
NZ, NX, NC, NY = 8, 4, 2, 4
norm_eps = 1e-05
BF, F32 = jnp.bfloat16, jnp.float32
MESH = pl.DeviceIdType.MESH

CHUNKS = ((0, 0), (1, 0), (0, 1), (1, 1), (2, 0), (2, 1))
NQ = len(CHUNKS)
ROWS, WIDTH = 768, 2048
BLOCK = ROWS // NZ
EARLY = 3
PASSES = 4
PIECE = WIDTH // PASSES
BY_X = PIECE // NX
NP = 2
PART = ROWS // NC // NP
SHARE = BLOCK // NC
ORDER = (
    "A0 K1 K2 K3", "R0 A1 K4 K5", "A2 X0 R1 A3", "R2", "X1 A4 R3 X2", "Z0 A5 Q0,0 R4",
    "X3 Q0,1 Q0,7 Z1", "R5 Q1,0 X4 Q0,2", "Q0,6 X5 Z2 Q1,1", "Q1,7 Q0,3 Q0,5 N0",
    "Z3 Q1,2 Q1,6 N1", "Q0,4 Z4 N2 N3", "Q1,3 Q1,5 F0", "Z5 Q2,0 N4 N5",
    "Q1,4 Q2,1 Q2,7 N6", "Q2,2 Q2,6 N7 N8", "Q2,3 Q2,5 N9 N10", "F1 Q2,4 N11 P0",
    "S3 F2 P1", "H0,0 H0,1", "F3 T0 T1 P2", "P3 H1,0 U0 T2",
    "H1,1 U1 T3", "V0 B0,0 B0,1 U2", "C0,0 C0,1 V1 B1,0",
    "B1,1 U3 D0,0 C1,0", "D0,1 C1,1 V2", "B2,0 B2,1 E0,0 V3",
    "B3,0 B3,1 D1,0 E0,1", "C2,0 D1,1 C2,1 C3,0", "C3,1 E1,0 D2,0 G0",
    "E1,1 D2,1 D3,0 D3,1", "E2,0 G1 E2,1 E3,0", "E3,1 G2 G3",
)


def send(src, dst, send_sem, recv_sem, to):
    pltpu.make_async_remote_copy(
        src_ref=src, dst_ref=dst, send_sem=send_sem, recv_sem=recv_sem, device_id=to, device_id_type=MESH
    ).start()


def wait_bytes(ref, sem):
    pltpu.make_async_copy(ref, ref, sem).wait()


def kernel(
    tokens, ids_in, mix_in, gain_in, gate, up, down,
    og, ou, od, out,
    ids, mix, gain, mat, tok, xs, ar, fw, xr, ts, w, xn, gates, h,
    pb, own, r1, s1, t2, u2, r2, s2, r3, s4, r4,
    in_sem, a_send, a_recv, f_send, f_recv, x_send, x_recv, z_send, z_recv, n_recv,
    c_send, c_recv, g_send, g_recv, o_sem,
    send1, recv1, send2, recv2, sendt, recvt, send3, recv3, send4, recv4,
):
    z, x, c, y = (lax.axis_index(a) for a in ("fs_0", "fs_1", "fs_2", "tp"))
    me = 2 * x + c
    ahead, behind, across = (lax.rem(y + o, NY) for o in (1, 3, 2))
    right, left, opposite = (lax.rem(x + o, NX) for o in (1, 3, 2))
    column = pl.multiple_of(256 * z, 256)

    pairs = ((gain_in, gain), (gate, mat.at[0]), (up, mat.at[1]), (down, mat.at[2]), (tokens, tok), (ids_in, ids), (mix_in, mix))
    reads = [pltpu.make_async_copy(src, dst, in_sem.at[n]) for n, (src, dst) in enumerate(pairs)]
    for r in reads[:2]:
        r.start()

    barrier = pltpu.get_barrier_semaphore()
    peers = []
    for off in range(1, NX * NC):
        j = lax.rem(me + off, NX * NC)
        peers.append({"fs_1": j // 2, "fs_2": lax.rem(j, 2)})
    for off in range(1, NZ):
        peers.append({"fs_0": lax.rem(z + off, NZ)})
    peers += [{"tp": ahead}, {"tp": behind}]
    for to in peers:
        pl.semaphore_signal(barrier, inc=1, device_id=to, device_id_type=MESH)

    def pack(q):
        m, el = CHUNKS[q]
        if q == 0:
            reads[0].wait()
        if el == 0:
            reads[1 + m].wait()
        if q == 0:
            for r in reads[2:]:
                r.start()
        low = lax.broadcasted_iota(jnp.int32, (32, 128), 1) < 64
        eye = lax.broadcasted_iota(jnp.int32, (32, 32), 0) == lax.broadcasted_iota(jnp.int32, (32, 32), 1)
        scale = jnp.sum(jnp.where(eye, gain[...], 0.0), axis=1, keepdims=True)

        def one(i, carry):
            ep, xp = i // NX, lax.rem(i, NX)
            at = pl.multiple_of(128 * xp, 128)
            a = mat[m, 2 * ep + el, :, pl.ds(at, 128)]
            b = mat[m, 2 * ep + el, :, pl.ds(pl.multiple_of(512 + at, 128), 128)]
            if m < 2:
                a, b = a * scale, b * scale
            xs[q, ep, 2 * xp] = jnp.where(low, a, pltpu.roll(b, 64, 1)).astype(BF)
            xs[q, ep, 2 * xp + 1] = jnp.where(low, pltpu.roll(a, 64, 1), b).astype(BF)
            return carry

        lax.fori_loop(0, 4 * NX, one, 0, unroll=4)

    def over_planes(q):
        send(xs.at[q, across, 0:4], fw.at[q, 0], a_send.at[q], f_recv.at[q, 0], {"tp": ahead})
        send(xs.at[q, across, 4:8], fw.at[q, 1], a_send.at[q], f_recv.at[q, 1], {"tp": behind})
        send(xs.at[q, ahead], ar.at[q, y], a_send.at[q], a_recv.at[q], {"tp": ahead})
        send(xs.at[q, behind], ar.at[q, y], a_send.at[q], a_recv.at[q], {"tp": behind})
        ar[q, y] = xs[q, y]

    def relay(q):
        wait_bytes(fw.at[q, 0], f_recv.at[q, 0])
        send(fw.at[q, 0], ar.at[q, behind, 0:4], f_send.at[q], a_recv.at[q], {"tp": ahead})
        wait_bytes(fw.at[q, 1], f_recv.at[q, 1])
        send(fw.at[q, 1], ar.at[q, ahead, 4:8], f_send.at[q], a_recv.at[q], {"tp": behind})

    def over_x(q):
        wait_bytes(ar.at[q, 0:3], a_recv.at[q])
        for off in range(1, NX * NC):
            j = lax.rem(me + off, NX * NC)
            send(
                ar.at[q, :, j], xr.at[q, me], x_send.at[q], x_recv.at[q],
                {"fs_1": j // 2, "fs_2": lax.rem(j, 2)},
            )
        xr[q, me] = ar[q, :, me]

    def over_z(q):
        wait_bytes(xr.at[q, 0:7], x_recv.at[q])

        def one(y0, carry):
            for half in range(2):
                rows = jnp.concatenate([xr[q, 4 * half + k, y0] for k in range(4)], axis=0)
                ts[q, y0, :, 128 * half : 128 * (half + 1)] = rows.T
            return carry

        lax.fori_loop(0, NY, one, 0)
        for off in (1, 7, 2, 6, 3, 5, 4) if q < EARLY else (4, 3, 5, 2, 6, 1, 7):
            zp = lax.rem(z + off, NZ)
            rows = pl.multiple_of(64 * lax.rem(zp, 2), 64)
            send(
                ts.at[q, zp // 2, pl.ds(rows, 64), :], w.at[q, y, :, pl.ds(column, 256)],
                z_send.at[q], n_recv.at[q, off] if q < EARLY else z_recv.at[q], {"fs_0": zp},
            )
        rows = pl.multiple_of(64 * lax.rem(z, 2), 64)
        w[q, y, :, pl.ds(column, 256)] = ts[q, z // 2, pl.ds(rows, 64), :]

    def spread_first(q, off):
        lanes = pl.ds(pl.multiple_of(256 * lax.rem(z + NZ - off, NZ), 256), 256)
        if off > 0:
            wait_bytes(w.at[q, 0, :, 0:256], n_recv.at[q, off])
        block = w.at[q, y, :, lanes]
        send(block, block, c_send.at[q], c_recv.at[q, 0], {"tp": ahead})
        send(block, block, c_send.at[q], c_recv.at[q, 1], {"tp": behind})

    def spread(q):
        wait_bytes(w.at[q, 0, :, 0:1792], z_recv.at[q])
        send(w.at[q, y], w.at[q, y], c_send.at[q], c_recv.at[q, 0], {"tp": ahead})
        send(w.at[q, y], w.at[q, y], c_send.at[q], c_recv.at[q, 1], {"tp": behind})

    def spread_on(q):
        wait_bytes(w.at[q, behind], c_recv.at[q, 0])
        send(w.at[q, behind, 0:32], w.at[q, behind, 0:32], g_send.at[q], g_recv.at[q], {"tp": ahead})
        wait_bytes(w.at[q, ahead], c_recv.at[q, 1])
        send(w.at[q, ahead, 32:64], w.at[q, ahead, 32:64], g_send.at[q], g_recv.at[q], {"tp": behind})

    def arrived(q):
        wait_bytes(w.at[q, across], g_recv.at[q])
        m, el = CHUNKS[q]
        for ep in range(NY):
            pltpu.make_async_copy(w.at[q, ep], (og, ou)[m].at[2 * ep + el], o_sem.at[q]).start()

    def piece(p, plane):
        return w.at[4:6, plane, :, PIECE * p : PIECE * (p + 1)]

    def spread_down(p):
        if p == 0:
            for q in (4, 5):
                wait_bytes(w.at[q, 0, :, 0:1792], z_recv.at[q])
        send(piece(p, y), piece(p, y), c_send.at[4 + p], c_recv.at[4 + p, 0], {"tp": ahead})
        send(piece(p, y), piece(p, y), c_send.at[4 + p], c_recv.at[4 + p, 1], {"tp": behind})

    def spread_down_on(p):
        wait_bytes(piece(p, behind), c_recv.at[4 + p, 0])
        part = piece(p, behind).at[0]
        send(part, part, g_send.at[4 + p], g_recv.at[4 + p], {"tp": ahead})
        wait_bytes(piece(p, ahead), c_recv.at[4 + p, 1])
        part = piece(p, ahead).at[1]
        send(part, part, g_send.at[4 + p], g_recv.at[4 + p], {"tp": behind})

    def arrived_down(p):
        wait_bytes(piece(p, across), g_recv.at[4 + p])
        lanes = slice(PIECE * p, PIECE * (p + 1))
        for ep in range(NY):
            for el in range(2):
                pltpu.make_async_copy(
                    w.at[4 + el, ep, :, lanes], od.at[2 * ep + el, :, lanes], o_sem.at[4 + p]
                ).start()

    def normalize(i):
        if i == 0:
            for r in reads[4:]:
                r.wait()
            expert = lax.broadcasted_iota(jnp.int32, (8, ROWS), 0)
            by_expert = jnp.where(ids[0:1, :] == expert, mix[0:1, :], 0.0)
            by_expert = by_expert + jnp.where(ids[1:2, :] == expert, mix[1:2, :], 0.0)
            gates[...] = by_expert.T

        def one(j, carry):
            rows = pl.ds(pl.multiple_of(64 * i + 16 * j, 16), 16)
            v = tok[rows, :].astype(F32)
            v = v - jnp.mean(v, axis=1, keepdims=True)
            var = jnp.mean(v * v, axis=1, keepdims=True)
            xn[rows, :] = (v * lax.rsqrt(var + norm_eps)).astype(BF)
            return carry

        lax.fori_loop(0, 4, one, 0, unroll=4)

    contract = (((1,), (1,)), ((), ()))

    def hide(el, i):
        rows = pl.ds(NC * PART * i, NC * PART)
        v = xn[rows, :]
        low = lax.broadcasted_iota(jnp.int32, (NC * PART, 128), 1) < 64
        first = 2 * el
        for pair in range(2):
            wg = w[first, 2 * pair : 2 * pair + 2].reshape(128, WIDTH)
            wu = w[first + 1, 2 * pair : 2 * pair + 2].reshape(128, WIDTH)
            g = lax.dot_general(v, wg, contract, preferred_element_type=F32)
            u = lax.dot_general(v, wu, contract, preferred_element_type=F32)
            e = 4 * pair + el
            share = jnp.where(low, gates[rows, e : e + 1], gates[rows, e + 2 : e + 3])
            hid = (g / (1.0 + jnp.exp(-g)) * u * share).astype(BF)
            at = 256 * el + 128 * pair
            for b in range(NZ // NP):
                for core in range(NC):
                    h[core, PART * i + SHARE * b : PART * i + SHARE * (b + 1), at : at + 128] = hid[
                        BLOCK * b + SHARE * core : BLOCK * b + SHARE * (core + 1)
                    ]

    def side_of(k):
        return lax.rem(z // 4 + 1 - k, NP)

    def part(s, k, core):
        v = h[core, pl.ds(pl.multiple_of(PART * side_of(k), PART), PART), :]
        lanes = slice(PIECE * s, PIECE * (s + 1))
        a = w[4, :, :, lanes].reshape(256, PIECE)
        b = w[5, :, :, lanes].reshape(256, PIECE)
        return jnp.dot(v[:, 0:256], a, preferred_element_type=F32) + jnp.dot(
            v[:, 256:512], b, preferred_element_type=F32
        )

    def between_cores(s, k):
        i = NP * s + k
        pb[i] = part(s, k, 1 - c).astype(BF)
        send(pb.at[i], r1.at[i], send1.at[i], recv1.at[i], {"fs_2": 1 - c})
        own[i] = part(s, k, c)

    def sum_x(s, k):
        i = NP * s + k
        wait_bytes(r1.at[i], recv1.at[i])
        total = (own[i] + r1[i].astype(F32)).astype(BF)
        for xp in range(NX):
            for half in range(2):
                s1[i, xp, half] = total[BLOCK * half : BLOCK * (half + 1), BY_X * xp : BY_X * (xp + 1)]
        send(s1.at[i, opposite, 0], t2.at[i, 0], sendt.at[i], recvt.at[i, 0], {"fs_1": right})
        send(s1.at[i, opposite, 1], t2.at[i, 1], sendt.at[i], recvt.at[i, 1], {"fs_1": left})
        send(s1.at[i, right, 1], r2.at[i, 1, 1], send2.at[i], recv2.at[i], {"fs_1": right})
        send(s1.at[i, left, 0], r2.at[i, 0, 1], send2.at[i], recv2.at[i], {"fs_1": left})

    def sum_x_on(s, k):
        i = NP * s + k
        wait_bytes(t2.at[i, 0], recvt.at[i, 0])
        u2[i, 0] = (s1[i, right, 0].astype(F32) + t2[i, 0].astype(F32)).astype(BF)
        send(u2.at[i, 0], r2.at[i, 0, 0], send2.at[i], recv2.at[i], {"fs_1": right})
        wait_bytes(t2.at[i, 1], recvt.at[i, 1])
        u2[i, 1] = (s1[i, left, 1].astype(F32) + t2[i, 1].astype(F32)).astype(BF)
        send(u2.at[i, 1], r2.at[i, 1, 0], send2.at[i], recv2.at[i], {"fs_1": left})

    def sum_z(s, k):
        i = NP * s + k
        wait_bytes(r2.at[i], recv2.at[i])
        for half in range(2):
            total = s1[i, x, half].astype(F32) + (r2[i, half, 0].astype(F32) + r2[i, half, 1].astype(F32))
            for two in range(2):
                s2[i, 2 * half + two] = total[SHARE * two : SHARE * (two + 1)].astype(BF)
        here = lax.rem(z, 4)
        for step in range(k, 4):
            b = lax.rem(here + step, 4)
            send(s2.at[i, b], r3.at[s, z], send3.at[i], recv3.at[s], {"fs_0": 4 * side_of(k) + b})
        if k == 1:
            r3[s, z] = s2[i, here]

    amid = x // 2 == c

    def give_rows(s):
        wait_bytes(r3.at[s, 0:7], recv3.at[s])
        total = r3[s, 0].astype(F32)
        for i in range(1, NZ):
            total = total + r3[s, i].astype(F32)
        row = lax.broadcasted_iota(jnp.int32, (64, SHARE), 0)
        col = lax.broadcasted_iota(jnp.int32, (64, SHARE), 1)
        within = lax.rem(row, 16)
        pick = ((col == (row // 16) * 12 + within) & (within < 12)).astype(BF)
        got = jnp.dot(pick, total.astype(BF), preferred_element_type=F32).astype(BF)
        for i in range(4):
            s4[s, i] = got[16 * i : 16 * (i + 1)]
        lanes = pl.ds(pl.multiple_of(PIECE * s + BY_X * x, BY_X), BY_X)

        def give(i):
            j = 4 * c + i
            send(
                s4.at[s, i], r4.at[:, lanes], send4.at[s], recv4.at[s],
                {"fs_1": j // 2, "fs_2": lax.rem(j, 2)},
            )

        first = lax.rem(me, 4)
        for step in range(1, 4):
            give(lax.rem(first + step, 4))

        @pl.when(amid)
        def _():
            r4[:, lanes] = s4[s, first]

        @pl.when(jnp.logical_not(amid))
        def _():
            give(first)

    def wait_rows(s, sem):
        @pl.when(amid)
        def _():
            wait_bytes(r4.at[:, 0 : 3 * BY_X], sem.at[s])

        @pl.when(jnp.logical_not(amid))
        def _():
            wait_bytes(r4.at[:, 0 : 4 * BY_X], sem.at[s])

    pack(0)
    pl.semaphore_wait(barrier, len(peers))
    names = dict(
        K=pack, A=over_planes, R=relay, X=over_x, Z=over_z, Q=spread_first, S=spread, F=spread_on, P=arrived, N=normalize, H=hide,
        T=spread_down, U=spread_down_on, V=arrived_down,
        B=between_cores, C=sum_x, D=sum_x_on, E=sum_z, G=give_rows,
    )
    for line in ORDER:
        for step in line.split():
            name, args = step[0], step[1:].split(",")
            names[name](*(int(a) for a in args))

    for q in range(NQ):
        wait_bytes(ar.at[q, 0:3], a_send.at[q])
        wait_bytes(fw.at[q], f_send.at[q])
        wait_bytes(xr.at[q, 0:7], x_send.at[q])
        wait_bytes(w.at[q, 0, :, 0:1792], z_send.at[q])
    for q in range(4):
        wait_bytes(w.at[q, 0:2], c_send.at[q])
        wait_bytes(w.at[q, 0], g_send.at[q])
        wait_bytes(w.at[q], o_sem.at[q])
    for p in range(PASSES):
        wait_bytes(w.at[4, :, :, 0:PIECE], c_send.at[4 + p])
        wait_bytes(piece(p, 0), g_send.at[4 + p])
        wait_bytes(w.at[4:6, :, :, 0:PIECE], o_sem.at[4 + p])
    for s in range(PASSES):
        for k in range(NP):
            i = NP * s + k
            wait_bytes(pb.at[i], send1.at[i])
            wait_bytes(t2.at[i], sendt.at[i])
            wait_bytes(r2.at[i], send2.at[i])
            wait_bytes(s2.at[i, k:4], send3.at[i])
        wait_rows(s, recv4)
    out[...] = r4[0:12, :]
    for s in range(PASSES):
        wait_rows(s, send4)


def run(*args):
    weights = jax.ShapeDtypeStruct((8, 64, WIDTH), BF)
    vmem = pl.BlockSpec(memory_space=pltpu.VMEM)
    hbm = pl.BlockSpec(memory_space=pl.ANY)
    dma = pltpu.SemaphoreType.DMA
    return pl.pallas_call(
        kernel,
        out_shape=(weights, weights, weights, jax.ShapeDtypeStruct((12, WIDTH), BF)),
        in_specs=[hbm] * 7,
        out_specs=(hbm, hbm, hbm, vmem),
        scratch_shapes=[
            pltpu.VMEM((2, ROWS), jnp.int32),
            pltpu.VMEM((2, ROWS), F32),
            pltpu.VMEM((1, 32), F32),
            pltpu.VMEM((3, 8, 32, 1024), F32),
            pltpu.VMEM((ROWS, WIDTH), BF),
            pltpu.VMEM((NQ, NY, 8, 32, 128), BF),
            pltpu.VMEM((NQ, NY, 8, 32, 128), BF),
            pltpu.VMEM((NQ, 2, 4, 32, 128), BF),
            pltpu.VMEM((NQ, 8, NY, 32, 128), BF),
            pltpu.VMEM((NQ, NY, 128, 256), BF),
            pltpu.VMEM((NQ, NY, 64, WIDTH), BF),
            pltpu.VMEM((ROWS, WIDTH), BF),
            pltpu.VMEM((ROWS, 8), F32),
            pltpu.VMEM((NC, ROWS // NC, 512), BF),
            pltpu.VMEM((PASSES * NP, PART, PIECE), BF),
            pltpu.VMEM((PASSES * NP, PART, PIECE), F32),
            pltpu.VMEM((PASSES * NP, PART, PIECE), BF),
            pltpu.VMEM((PASSES * NP, NX, 2, BLOCK, BY_X), BF),
            pltpu.VMEM((PASSES * NP, 2, BLOCK, BY_X), BF),
            pltpu.VMEM((PASSES * NP, 2, BLOCK, BY_X), BF),
            pltpu.VMEM((PASSES * NP, 2, 2, BLOCK, BY_X), BF),
            pltpu.VMEM((PASSES * NP, 4, SHARE, BY_X), BF),
            pltpu.VMEM((PASSES, NZ, SHARE, BY_X), BF),
            pltpu.VMEM((PASSES, 4, 16, BY_X), BF),
            pltpu.VMEM((16, WIDTH), BF),
            dma((7,)),
            dma((NQ,)), dma((NQ,)),
            dma((NQ,)), dma((NQ, 2)),
            dma((NQ,)), dma((NQ,)),
            dma((NQ,)), dma((NQ,)), dma((EARLY, NZ)),
            dma((4 + PASSES,)), dma((4 + PASSES, 2)),
            dma((4 + PASSES,)), dma((4 + PASSES,)),
            dma((4 + PASSES,)),
            dma((PASSES * NP,)), dma((PASSES * NP,)),
            dma((PASSES * NP,)), dma((PASSES * NP,)),
            dma((PASSES * NP,)), dma((PASSES * NP, 2)),
            dma((PASSES * NP,)), dma((PASSES,)),
            dma((PASSES,)), dma((PASSES,)),
        ],
        compiler_params=pltpu.CompilerParams(
            collective_id=0, has_side_effects=True, vmem_limit_bytes=40 * 1024 * 1024
        ),
        name="hand_over_and_serve",
    )(*args)


def put_kernel(wg, wu, wd, small, og, ou, od, out, sems):
    hops = [(small, out)]
    for w, o in ((wg, og), (wu, ou), (wd, od)):
        for i in range(4):
            two = slice(2 * i, 2 * i + 2)
            hops.append((w.at[two], o.at[two]))
    writes = [pltpu.make_async_copy(a, o, sems.at[n]) for n, (a, o) in enumerate(hops)]
    for copy in writes:
        copy.start()
    for copy in writes:
        copy.wait()


def put_out(*results):
    weights = jax.ShapeDtypeStruct((8, 64, WIDTH), BF)
    small = jax.ShapeDtypeStruct((12, WIDTH), BF)
    hbm = pl.BlockSpec(memory_space=pl.ANY)
    vmem = pl.BlockSpec(memory_space=pltpu.VMEM)
    return pl.pallas_call(
        put_kernel,
        out_shape=(weights, weights, weights, small),
        in_specs=[vmem] * 4,
        out_specs=(hbm, hbm, hbm, hbm),
        scratch_shapes=[pltpu.SemaphoreType.DMA((13,))],
        compiler_params=pltpu.CompilerParams(vmem_limit_bytes=16 * 1024 * 1024),
        name="put_out",
    )(*results)


def local(tokens, norm_gain, gate_weight, up_weight, down_weight, expert_ids, expert_mix):
    args = (
        tokens.reshape(ROWS, WIDTH), expert_ids.reshape(ROWS, 2).T, expert_mix.reshape(ROWS, 2).T,
        norm_gain.reshape(1, 32), gate_weight, up_weight, down_weight,
    )
    results = run(*(pltpu.with_memory_space_constraint(a, pltpu.HBM) for a in args))
    gate_t, up_t, down_t, mixed = put_out(*results)
    turned = tuple(jnp.swapaxes(t, 1, 2) for t in (gate_t, up_t, down_t))
    return turned + (mixed.reshape(12, 1, WIDTH),)


def solution(mesh):
    finer = Mesh(mesh.devices.reshape(NZ, NX, NC, NY), ("fs_0", "fs_1", "fs_2", "tp"))
    placed = (
        P(None, "tp", None),
        P(FS),
        P(None, FS, "tp"),
        P(None, FS, "tp"),
        P(None, FS, "tp"),
        P(None, "tp", None),
        P(None, "tp", None),
    )
    return jax.shard_map(
        local,
        mesh=finer,
        in_specs=placed,
        out_specs=(P(None, None, FS), P(None, None, FS), P(None, None, FS), P(FS, "tp", None)),
        check_vma=False,
    )
```
